256 devices in a mesh: sp: 64 (over z, x, core), tp: 4 (over y).
Axes of the slice: x: 4, y: 4, z: 8, core: 2. Of those that a mesh axis runs over, the one named last changes fastest.
Arguments:
- x_res: bfloat16 [16384, 2048], P(('sp', 'tp')), may hold values from -6 to 6
- q_a: bfloat16 [16384, 1024], P('sp', 'tp'), may hold values from -48 to 48
- k_a: bfloat16 [16384, 256], P('sp', 'tp'), may hold values from -48 to 48
- v_a: bfloat16 [16384, 256], P('sp', 'tp'), may hold values from -6 to 6
- q_b: bfloat16 [16384, 1024], P('sp', 'tp'), may hold values from -48 to 48
- k_b: bfloat16 [16384, 512], P('sp', 'tp'), may hold values from -48 to 48
- v_b: bfloat16 [16384, 512], P('sp', 'tp'), may hold values from -6 to 6
- gain_qa: float32 [64], replicated, may hold values from 1.2 to 6
- gain_ka: float32 [64], replicated, may hold values from 1.2 to 6
- gain_qb: float32 [128], replicated, may hold values from 1.2 to 6
- gain_kb: float32 [128], replicated, may hold values from 1.2 to 6
- w_out_a: bfloat16 [1024, 2048], P('tp'), may hold values from -0.125 to 0.125
- w_out_b: bfloat16 [1024, 2048], P('tp'), may hold values from -0.125 to 0.125
- gain_mid: float32 [2048], replicated, may hold values from 0.1 to 1.9
- w_gate: bfloat16 [2048, 3072], P('sp', 'tp'), may hold values from -0.125 to 0.125
- w_up: bfloat16 [2048, 3072], P('sp', 'tp'), may hold values from -0.125 to 0.125
- conv_gate: float32 [3, 3072], P(None, 'tp'), may hold values from -3.5 to 3.5
- conv_up: float32 [3, 3072], P(None, 'tp'), may hold values from -3.5 to 3.5
- w_down: bfloat16 [3072, 2048], P('tp', 'sp'), may hold values from -0.109375 to 0.109375
Outputs:
- layer_out: bfloat16 [16384, 2048], P(('sp', 'tp'))
The draws below stay inside these ranges and needn't reach their ends.
All inputs are finite; a program needn't handle non-finite values.
Results may differ from the reference program's by a relative error of at most 0.014.
The reference program's roundings to bfloat16 on the way (of `qa_n`, `ka_n`, `qb_n`, `kb_n`, `normed`, `gate_pre`, `up_pre` and `hidden`) count: a program that leaves them out, or rounds other values in their place, can miss the bound.
Values may be sent and summed in bfloat16 or wider, within the bound.
A program may use at most 128 MiB of HBM per device.

```python
import jax
import jax.numpy as jnp
from jax import lax

D = 2048
FF = 3072
HQA = 16
HKVA = 4
DHA = 64
HQB = 8
HKVB = 4
DHB = 128
TOKENS = 16384
N_TP = 4


def drawn_keys(key, heads, head_size, salt):
    base = jax.random.fold_in(key, salt)
    streams = jax.random.split(base, 1)
    keys = jax.random.truncated_normal(streams[0], -4.0, 4.0, (TOKENS, heads, head_size), jnp.float32)
    return keys


def drawn_queries(key, heads, head_size, salt):
    queries = jax.random.truncated_normal(jax.random.fold_in(key, salt + 1), -4.0, 4.0, (TOKENS, heads, head_size), jnp.float32)
    return queries.reshape(TOKENS, heads * head_size).astype(jnp.bfloat16)


def drawn_gain(key, head_size, salt):
    gains = jax.random.uniform(jax.random.fold_in(key, salt), (head_size,), jnp.float32, 1.2, 2.4)
    return gains


def draw_q_a(key, part):
    return drawn_queries(key, HQA, DHA, 11)


def draw_k_a(key, part):
    keys = drawn_keys(key, HKVA, DHA, 11)
    return keys.reshape(TOKENS, HKVA * DHA).astype(jnp.bfloat16)


def draw_q_b(key, part):
    return drawn_queries(key, HQB, DHB, 21)


def draw_k_b(key, part):
    keys = drawn_keys(key, HKVB, DHB, 21)
    return keys.reshape(TOKENS, HKVB * DHB).astype(jnp.bfloat16)


def draw_gain_qa(key, part):
    return drawn_gain(key, DHA, 31)


def draw_gain_ka(key, part):
    return drawn_gain(key, DHA, 32)


def draw_gain_qb(key, part):
    return drawn_gain(key, DHB, 33)


def draw_gain_kb(key, part):
    return drawn_gain(key, DHB, 34)


def steps_of(rng, extent, pieces, low, top_value):
    def one(axis_at, blocks):
        heights = jax.random.uniform(jax.random.fold_in(jax.random.fold_in(rng, 6), axis_at), (blocks,), jnp.float32, low / len(pieces), top_value / len(pieces))
        return jnp.repeat(jnp.exp(heights), extent[axis_at] // blocks).reshape((-1,) + (1,) * (len(extent) - axis_at - 1))

    level = one(*pieces[0])
    for cut in pieces[1:]:
        level = level * one(*cut)
    return level


def noise(rng, extent, deviation, bound, cuts=(), held_as=jnp.bfloat16):
    level = steps_of(rng, extent, cuts, -0.22, 0.18) if cuts else 1.0
    values = jax.random.normal(rng, extent, jnp.float32) * deviation * level
    return jnp.minimum(jnp.maximum(values, -bound), bound).astype(held_as)


def setup_inputs(seed: int = 0) -> dict:
    streams_of = jax.random.split(jax.random.key(seed), 20)
    return {
        "x_res": noise(streams_of[0], (TOKENS, D), 1.0, 6.0, ((0, 256),)),
        "q_a": draw_q_a(jax.random.fold_in(streams_of[19], 71), 0),
        "k_a": draw_k_a(jax.random.fold_in(streams_of[19], 71), 0),
        "v_a": noise(streams_of[3], (TOKENS, HKVA * DHA), 1.0, 6.0, ((0, 64), (1, 4))),
        "q_b": draw_q_b(jax.random.fold_in(streams_of[19], 71), 0),
        "k_b": draw_k_b(jax.random.fold_in(streams_of[19], 71), 0),
        "v_b": noise(streams_of[6], (TOKENS, HKVB * DHB), 1.0, 6.0, ((0, 64), (1, 4))),
        "gain_qa": draw_gain_qa(jax.random.fold_in(streams_of[19], 71), 0),
        "gain_ka": draw_gain_ka(jax.random.fold_in(streams_of[19], 71), 0),
        "gain_qb": draw_gain_qb(jax.random.fold_in(streams_of[19], 71), 0),
        "gain_kb": draw_gain_kb(jax.random.fold_in(streams_of[19], 71), 0),
        "w_out_a": noise(streams_of[11], (HQA * DHA, D), (HQA * DHA + HQB * DHB) ** -0.5, 0.125, ((0, 4),)),
        "w_out_b": noise(streams_of[12], (HQB * DHB, D), (HQA * DHA + HQB * DHB) ** -0.5, 0.125, ((0, 4),)),
        "gain_mid": jnp.clip(1.0 + 0.18 * jax.random.normal(streams_of[13], (D,), jnp.float32), 0.1, 1.9),
        "w_gate": noise(streams_of[14], (D, FF), D ** -0.5, 0.125, ((0, 64), (1, 4))),
        "w_up": noise(streams_of[15], (D, FF), D ** -0.5, 0.125, ((0, 64), (1, 4))),
        "conv_gate": noise(streams_of[16], (3, FF), 3 ** -0.5, 3.5, ((1, 4),), jnp.float32),
        "conv_up": noise(streams_of[17], (3, FF), 3 ** -0.5, 3.5, ((1, 4),), jnp.float32),
        "w_down": noise(streams_of[18], (FF, D), FF ** -0.5, 0.109375, ((0, 4), (1, 64))),
    }


norm_eps = 1e-06
rope_theta = 10000.0

def rotary_angles(positions, head_size):
    half = head_size // 2
    inverse = jnp.power(jnp.float32(rope_theta), -jnp.arange(0, half, 2, dtype=jnp.float32) / half)
    grid_row = (positions // 64).astype(jnp.float32)[:, None] * inverse[None, :]
    grid_col = (positions % 64).astype(jnp.float32)[:, None] * inverse[None, :]
    angles = jnp.concatenate([grid_row, grid_row, grid_col, grid_col], axis=-1)
    return (jnp.cos(angles), jnp.sin(angles))

def rotate_half(values):
    first, second = jnp.split(values, 2, axis=-1)
    return jnp.concatenate([-second, first], axis=-1)

def prepare(raw, gain, head_size, positions):
    count = raw.shape[0]
    heads = raw.shape[1] // head_size
    values = raw.astype(jnp.float32).reshape(count, heads, head_size)
    values = values * lax.rsqrt(lax.optimization_barrier(jnp.mean(values * values, axis=-1, keepdims=True)) + norm_eps)
    values = values * gain.astype(jnp.float32)
    cosine, sine = rotary_angles(positions, head_size)
    row_part, col_part = jnp.split(values, 2, axis=-1)
    turned = jnp.concatenate([rotate_half(row_part), rotate_half(col_part)], axis=-1)
    values = values * cosine[:, None, :] + turned * sine[:, None, :]
    return values.astype(jnp.bfloat16)

def attention_group(queries, keys, values, head_size):
    count = queries.shape[0]
    kv_heads = keys.shape[1]
    groups = queries.shape[1] // kv_heads
    block = 256 if count % 256 == 0 else 64
    blocked = queries.reshape(count // block, block, kv_heads, groups, head_size)
    keys_f = keys.astype(jnp.float32)
    values_f = values.astype(jnp.float32)
    scale = jnp.float32(head_size ** (-0.5))

    def one_block(query_block):
        scores = jnp.einsum('qkgd,skd->kgqs', query_block.astype(jnp.float32), keys_f) * scale
        top = lax.optimization_barrier(jnp.max(scores, axis=-1, keepdims=True))
        expd = jnp.exp(scores - top)
        totals = lax.optimization_barrier(jnp.sum(expd, axis=-1))
        weights = expd.astype(jnp.bfloat16).astype(jnp.float32)
        summed = jnp.einsum('kgqs,skd->kgqd', weights, values_f) / totals[..., None]
        return jnp.transpose(summed, (2, 0, 1, 3)).reshape(block, kv_heads * groups * head_size).astype(jnp.bfloat16)
    result = lax.map(one_block, blocked)
    return result.reshape(count, kv_heads * groups * head_size)

def reference(x_res, q_a, k_a, v_a, q_b, k_b, v_b, gain_qa, gain_ka, gain_qb, gain_kb, w_out_a, w_out_b, gain_mid, w_gate, w_up, conv_gate, conv_up, w_down):
    count = x_res.shape[0]
    positions = jnp.arange(count, dtype=jnp.int32)
    qa_n = prepare(q_a, gain_qa, DHA, positions)
    ka_n = prepare(k_a, gain_ka, DHA, positions)
    qb_n = prepare(q_b, gain_qb, DHB, positions)
    kb_n = prepare(k_b, gain_kb, DHB, positions)
    va_h = v_a.reshape(count, HKVA, DHA)
    vb_h = v_b.reshape(count, HKVB, DHB)
    attn_a = attention_group(qa_n, ka_n, va_h, DHA)
    attn_b = attention_group(qb_n, kb_n, vb_h, DHB)
    width_a = HQA * DHA // N_TP
    width_b = HQB * DHB // N_TP
    projected = jnp.zeros((count, D), jnp.float32)
    for block in range(N_TP):
        partial_value = jnp.dot(attn_a[:, block * width_a:(block + 1) * width_a], w_out_a[block * width_a:(block + 1) * width_a], preferred_element_type=jnp.float32)
        partial_value = partial_value + jnp.dot(attn_b[:, block * width_b:(block + 1) * width_b], w_out_b[block * width_b:(block + 1) * width_b], preferred_element_type=jnp.float32)
        projected = projected + partial_value.astype(jnp.bfloat16).astype(jnp.float32)
    mid = x_res.astype(jnp.float32) + projected
    normed = mid * lax.rsqrt(lax.optimization_barrier(jnp.mean(mid * mid, axis=-1, keepdims=True)) + norm_eps)
    normed = (normed * gain_mid.astype(jnp.float32)).astype(jnp.bfloat16)
    gate_pre = jnp.dot(normed, w_gate, preferred_element_type=jnp.float32).astype(jnp.bfloat16)
    up_pre = jnp.dot(normed, w_up, preferred_element_type=jnp.float32).astype(jnp.bfloat16)

    def convolve(projected_rows, taps):
        padded = jnp.pad(projected_rows.astype(jnp.float32), ((1, 1), (0, 0)))
        taps = taps.astype(jnp.float32)
        return padded[:-2] * taps[0] + padded[1:-1] * taps[1] + padded[2:] * taps[2]
    gate_conv = convolve(gate_pre, conv_gate)
    up_conv = convolve(up_pre, conv_up)
    hidden = (jax.nn.silu(gate_conv) * up_conv).astype(jnp.bfloat16)
    width_f = FF // N_TP
    down = jnp.zeros((count, D), jnp.float32)
    for block in range(N_TP):
        partial_value = jnp.dot(hidden[:, block * width_f:(block + 1) * width_f], w_down[block * width_f:(block + 1) * width_f], preferred_element_type=jnp.float32)
        down = down + partial_value.astype(jnp.bfloat16).astype(jnp.float32)
    return (mid + down).astype(jnp.bfloat16)
```

```python
import functools
import math

import jax
import jax.numpy as jnp
from jax import lax
from jax.experimental import pallas as pl
from jax.experimental.pallas import tpu as pltpu
from jax.sharding import PartitionSpec as P

DHA = 64
DHB = 128
NZ = 8
NX = 4
NY = 4
NSETS = NZ
MESH = pl.DeviceIdType.MESH
F32 = jnp.float32
BF16 = jnp.bfloat16
LOG2E = math.log2(math.e)

norm_eps = 1e-06
rope_theta = 10000.0


def rotary_angles(positions, head_size):
    half = head_size // 2
    inverse = jnp.power(jnp.float32(rope_theta), -jnp.arange(0, half, 2, dtype=jnp.float32) / half)
    grid_row = (positions // 64).astype(jnp.float32)[:, None] * inverse[None, :]
    grid_col = (positions % 64).astype(jnp.float32)[:, None] * inverse[None, :]
    angles = jnp.concatenate([grid_row, grid_row, grid_col, grid_col], axis=-1)
    return (jnp.cos(angles), jnp.sin(angles))


def rotate_half(values):
    first, second = jnp.split(values, 2, axis=-1)
    return jnp.concatenate([-second, first], axis=-1)


def prepare(raw, gain, head_size, positions):
    count = raw.shape[0]
    heads = raw.shape[1] // head_size
    values = raw.astype(jnp.float32).reshape(count, heads, head_size)
    values = values * lax.rsqrt(jnp.mean(values * values, axis=-1, keepdims=True) + norm_eps)
    values = values * gain
    cosine, sine = rotary_angles(positions, head_size)
    row_part, col_part = jnp.split(values, 2, axis=-1)
    turned = jnp.concatenate([rotate_half(row_part), rotate_half(col_part)], axis=-1)
    values = values * cosine[:, None, :] + turned * sine[:, None, :]
    return values.astype(jnp.bfloat16)


class Place:
    def __init__(self):
        self.sp = lax.axis_index("sp")
        self.y = lax.axis_index("tp")
        self.c = self.sp % 2
        self.x = (self.sp // 2) % NX
        self.z = self.sp // (2 * NX)
        self.s = 1 - 2 * self.c

    def at(self, z, x, c):
        return (z * NX + x) * 2 + c

    def zz(self, d):
        return (self.z + d + 2 * NZ) % NZ

    def xx(self, d):
        return (self.x + d + 2 * NX) % NX

    def set_z(self, t, s):
        k = (t + 1) // 2
        sign = 1 - 2 * (t % 2)
        return self.zz(sign * s * k)


class Gather:
    def __init__(self, place, group_a, piece_a, piece_b, sems):
        self.p = place
        self.group_a, self.piece_a, self.piece_b = group_a, piece_a, piece_b
        (self.ax_s, self.ax_r, self.az_s, self.az_r, self.at_s, self.at_r,
         self.bz_s, self.bz_r, self.bx_s, self.bx_r, self.bt_s, self.bt_r) = sems

    def _copy(self, ref, s_sem, r_sem, sp):
        return pltpu.make_async_remote_copy(
            src_ref=ref, dst_ref=ref, send_sem=s_sem, recv_sem=r_sem,
            device_id={"sp": sp}, device_id_type=MESH,
        )

    def c_ax(self, k):
        p = self.p
        src_x = [p.x, p.xx(-p.s), p.x][k]
        to = [p.xx(p.s), p.xx(p.s), p.xx(-p.s)][k]
        return self._copy(self.piece_a(p.z, src_x, p.c), self.ax_s.at[k], self.ax_r.at[k], p.at(p.z, to, p.c))

    def c_az(self, t, to_z, src_z):
        p = self.p
        return self._copy(self.group_a(src_z, p.c), self.az_s.at[t], self.az_r.at[t], p.at(to_z, p.x, p.c))

    def c_at(self, t):
        p = self.p
        return self._copy(self.group_a(p.set_z(t, p.s), p.c), self.at_s.at[t], self.at_r.at[t], p.at(p.z, p.x, 1 - p.c))

    def c_bz(self, t, to_z, src_z):
        p = self.p
        return self._copy(self.piece_b(src_z, p.x, p.c), self.bz_s.at[t], self.bz_r.at[t], p.at(to_z, p.x, p.c))

    def c_bx(self, t, k):
        p = self.p
        src_x = [p.x, p.xx(-p.s), p.x][k]
        to = [p.xx(p.s), p.xx(p.s), p.xx(-p.s)][k]
        return self._copy(self.piece_b(p.set_z(t, p.s), src_x, p.c), self.bx_s.at[t, k], self.bx_r.at[t, k],
                          p.at(p.z, to, p.c))

    def c_bt(self, t, k):
        p = self.p
        src_x = [p.x, p.xx(-p.s), p.xx(p.s), p.xx(-2 * p.s)][k]
        return self._copy(self.piece_b(p.set_z(t, p.s), src_x, p.c), self.bt_s.at[t, k], self.bt_r.at[t, k],
                          p.at(p.z, p.x, 1 - p.c))

    def start_b(self):
        p = self.p
        self.c_bz(1, p.zz(p.s), p.z).start()
        self.c_bz(2, p.zz(-p.s), p.z).start()
        self.c_bx(0, 0).start()
        self.c_bx(0, 2).start()
        self.c_bt(0, 0).start()

    def start_a(self):
        self.c_ax(0).start()
        self.c_ax(2).start()

    def x_a(self):
        p = self.p
        self.c_ax(0).wait_recv()
        self.c_ax(1).start()
        self.c_ax(2).wait_recv()
        self.c_ax(1).wait_recv()
        self.c_az(1, p.zz(p.s), p.z).start()
        self.c_az(2, p.zz(-p.s), p.z).start()
        self.c_at(0).start()

    def _hop(self, t, copy):
        p = self.p
        sign = (2 * (t % 2) - 1) * p.s
        copy(t, p.z, p.set_z(t, p.s)).wait_recv()

        @pl.when(t <= NSETS - 3)
        def _():
            copy(t + 2, p.zz(sign), p.set_z(t, p.s)).start()

    def z_b(self, t):
        self._hop(t, self.c_bz)
        self.c_bx(t, 0).start()
        self.c_bx(t, 2).start()
        self.c_bt(t, 0).start()

    def z_a(self, t):
        self._hop(t, self.c_az)
        self.c_at(t).start()

    def x1(self, t):
        self.c_bx(t, 0).wait_recv()
        self.c_bx(t, 1).start()
        self.c_bt(t, 1).start()

    def x2(self, t):
        self.c_bx(t, 2).wait_recv()
        self.c_bt(t, 2).start()

    def x3(self, t):
        self.c_bx(t, 1).wait_recv()
        self.c_bt(t, 3).start()

    def arrived(self, t):
        self.c_at(t).wait_recv()
        for k in range(4):
            self.c_bt(t, k).wait_recv()

    def drain(self):
        p = self.p
        for k in range(3):
            self.c_ax(k).wait_send()

        @pl.loop(0, NSETS)
        def _(t):
            self.c_at(t).wait_send()
            for k in range(3):
                self.c_bx(t, k).wait_send()
            for k in range(4):
                self.c_bt(t, k).wait_send()

            @pl.when(t >= 1)
            def _():
                self.c_az(t, p.z, p.z).wait_send()
                self.c_bz(t, p.z, p.z).wait_send()


def gather_sems():
    d = pltpu.SemaphoreType.DMA
    return [d((3,)), d((3,)), d((8,)), d((8,)), d((8,)), d((8,)),
            d((8,)), d((8,)), d((8, 3)), d((8, 3)), d((8, 4)), d((8, 4))]


def dot(a, b):
    return jnp.dot(a, b, preferred_element_type=F32)


def kernel(kva_h, kvb_h, qa_ref, qb_ref, wgu_h, wd_h, woa_h, wob_h, x_ref, gain_ref, cg_ref, cu_ref, out_ref,
           ba, bb, wgu, wd, woa, wob, s_a, s_b, p_ref, acc_a, acc_b, mx,
           attn, part, rs_mid, rs_in, mid, ag, pre, halo, hid, part2, rs_mid2, rs_in2,
           loc, wo_sem, rs_s, rs_r, rs_s2, rs_r2, ag_s, ag_r, h_s, h_r, *sems):
    p = Place()
    n = len(sems) // 2

    barrier = pltpu.get_barrier_semaphore()
    up, down = (p.y + 1) % NY, (p.y + NY - 1) % NY
    opp = (p.y + 2) % NY
    sp_next, sp_prev = (p.sp + 1) % 64, (p.sp + 63) % 64
    own_a = pltpu.make_async_copy(kva_h, ba.at[p.c, p.z, p.x], loc.at[0])
    own_b = pltpu.make_async_copy(kvb_h, bb.at[p.c, p.z, p.x], loc.at[1])
    own_gu = pltpu.make_async_copy(wgu_h, wgu.at[p.z * NX + p.x, p.c], loc.at[2])
    own_d = pltpu.make_async_copy(wd_h, wd.at[p.z * NX + p.x, p.c], loc.at[3])
    own_oa = pltpu.make_async_copy(woa_h, woa, wo_sem.at[0])
    own_ob = pltpu.make_async_copy(wob_h, wob, wo_sem.at[1])
    for copy in (own_b, own_a, own_gu, own_d, own_oa, own_ob):
        copy.start()
    greeted = [p.at(p.zz(1), p.x, p.c), p.at(p.zz(-1), p.x, p.c), p.at(p.z, p.xx(1), p.c), p.at(p.z, p.xx(-1), p.c),
               p.at(p.z, p.x, 1 - p.c), sp_next, sp_prev]
    for sp in greeted:
        pl.semaphore_signal(barrier, inc=1, device_id={"sp": sp}, device_id_type=MESH)
    for y in (up, down):
        pl.semaphore_signal(barrier, inc=1, device_id={"tp": y}, device_id_type=MESH)
    pl.semaphore_wait(barrier, 9)

    g = Gather(p, lambda z, c: ba.at[c, z], lambda z, x, c: ba.at[c, z, x], lambda z, x, c: bb.at[c, z, x], sems[:n])
    w = Gather(p, lambda z, c: wgu.at[pl.ds(z * NX, NX), c], lambda z, x, c: wgu.at[z * NX + x, c],
               lambda z, x, c: wd.at[z * NX + x, c], sems[n:])

    own_b.wait()
    g.start_b()
    own_a.wait()
    g.start_a()
    own_gu.wait()
    own_d.wait()
    acc_a[...] = jnp.zeros_like(acc_a)
    acc_b[...] = jnp.zeros_like(acc_b)
    mx[...] = jnp.full_like(mx, -1e30)
    g.x_a()
    g.x1(0)
    g.x2(0)
    g.x3(0)
    g.arrived(0)

    zeros64 = jnp.zeros((64, 256), BF16)

    def scores(tile, buf, parts):
        top = None
        if tile < 4:
            q = qa_ref[tile]
            both = (jnp.concatenate([q, zeros64], axis=0), jnp.concatenate([zeros64, q], axis=0))
            for i, (cc, z) in enumerate(parts):
                keys = ba[cc, z, :, 0:128, :].reshape(512, 128)
                for h in range(2):
                    sc = dot(keys, both[h])
                    buf[pl.ds((i * 2 + h) * 512, 512), :] = sc
                    m8 = jnp.max(sc.reshape(64, 8, 256), axis=0)
                    top = m8 if top is None else jnp.maximum(top, m8)
        else:
            q = qb_ref[tile - 4]
            for i, (cc, z) in enumerate(parts):
                for h in range(2):
                    keys = bb[cc, z, 2 * h:2 * h + 2, 0:256, :].reshape(512, 128)
                    sc = dot(keys, q)
                    buf[pl.ds((i * 2 + h) * 512, 512), :] = sc
                    m8 = jnp.max(sc.reshape(64, 8, 256), axis=0)
                    top = m8 if top is None else jnp.maximum(top, m8)
        return jnp.max(top, axis=0, keepdims=True)

    def weigh(tile, buf, top, parts):
        scale = LOG2E if tile < 4 else LOG2E * DHB ** -0.5
        old = mx[tile]
        new = jnp.maximum(old, top * scale)
        mx[tile] = new
        factor = jnp.exp2(old - new)
        total = None
        for i, (cc, z) in enumerate(parts):
            for h in range(2):
                rows = pl.ds((i * 2 + h) * 512, 512)
                p_ref[rows, :] = jnp.exp2(buf[rows, :] * scale - new).astype(BF16)
                if tile < 4:
                    vt = jnp.concatenate([ba[cc, z, x, 128 + 64 * h:192 + 64 * h, :] for x in range(4)], axis=1)
                else:
                    vt = jnp.concatenate(
                        [bb[cc, z, x, 256 + 128 * e:384 + 128 * e, :] for x in (2 * h, 2 * h + 1) for e in range(2)], axis=1)
                vt = jnp.concatenate([vt, jnp.ones((16, 512), BF16)], axis=0)
                o = dot(vt, p_ref[rows, :])
                total = o if total is None else total + o
        if tile < 4:
            acc_a[tile] = acc_a[tile] * factor + total
        else:
            acc_b[tile - 4] = acc_b[tile - 4] * factor + total

    @pl.loop(1, NSETS + 1)
    def _(t):
        last = t == NSETS
        odd = t % 2 == 1
        parts = ((p.c, p.set_z(t - 1, p.s)), (1 - p.c, p.set_z(t - 1, -p.s)))

        @pl.when(odd)
        def _():
            g.z_b(t)

            @pl.when(t + 1 < NSETS)
            def _():
                g.z_b(t + 1)

        bufs = (s_a, s_b)
        top = scores(0, bufs[0], parts)
        for i in range(6):
            following = scores(i + 1, bufs[(i + 1) % 2], parts) if i < 5 else None
            weigh(i, bufs[i % 2], top, parts)
            top = following
            if i == 0:
                @pl.when(jnp.logical_not(last))
                def _():
                    g.x1(t)
            if i == 1:
                @pl.when(odd)
                def _():
                    g.z_a(t)

                    @pl.when(t + 1 < NSETS)
                    def _():
                        g.z_a(t + 1)
            if i == 2:
                @pl.when(jnp.logical_not(last))
                def _():
                    g.x2(t)
            if i == 3:
                @pl.when(jnp.logical_not(last))
                def _():
                    g.x3(t)
            if i == 5:
                @pl.when(jnp.logical_not(last))
                def _():
                    g.arrived(t)

    w.start_b()
    w.start_a()

    o_a = [acc_a[h, 0:64, :] / acc_a[h, 64:65, :] for h in range(4)]
    attn[:, 0:256] = jnp.concatenate(o_a, axis=0).T.astype(BF16)
    o_b = [acc_b[h, 0:128, :] / acc_b[h, 128:129, :] for h in range(2)]
    attn[:, 256:512] = jnp.concatenate(o_b, axis=0).T.astype(BF16)
    own_oa.wait()
    own_ob.wait()
    for k in range(8):
        cols = slice(k * 256, k * 256 + 256)
        tile = dot(attn[:, 0:256], woa[:, cols]) + dot(attn[:, 256:512], wob[:, cols])
        part[:, k // 4, :, (k % 4) * 256:(k % 4) * 256 + 256] = tile.astype(BF16).reshape(4, 64, 256)

    def to_y(src, dst, s_sem, r_sem, y):
        return pltpu.make_async_remote_copy(src_ref=src, dst_ref=dst, send_sem=s_sem, recv_sem=r_sem,
                                            device_id={"tp": y}, device_id_type=MESH)

    def reduce_copies(src, mids, ins, ss, rr):
        return (
            to_y(src.at[opp, 0], mids.at[0], ss.at[0], rr.at[0], up),
            to_y(src.at[opp, 1], mids.at[1], ss.at[1], rr.at[1], down),
            to_y(src.at[down, 0], ins.at[0], ss.at[2], rr.at[2], down),
            to_y(src.at[up, 1], ins.at[1], ss.at[3], rr.at[3], up),
            to_y(mids.at[2], ins.at[2], ss.at[4], rr.at[4], up),
            to_y(mids.at[3], ins.at[3], ss.at[5], rr.at[5], down),
        )

    def reduce_first(copies):
        for copy in copies[:4]:
            copy.start()

    def reduce_second(copies, src, mids):
        copies[0].wait_recv()
        mids[2] = (src[up, 0].astype(F32) + mids[0].astype(F32)).astype(BF16)
        copies[1].wait_recv()
        mids[3] = (src[down, 1].astype(F32) + mids[1].astype(F32)).astype(BF16)
        copies[4].start()
        copies[5].start()

    def reduce_last(copies):
        for copy in copies[2:]:
            copy.wait_recv()

    first = reduce_copies(part, rs_mid, rs_in, rs_s, rs_r)
    reduce_first(first)
    w.x_a()
    reduce_second(first, part, rs_mid)
    w.x1(0)
    w.x2(0)
    w.x3(0)
    w.arrived(0)
    reduce_last(first)

    def own_sum(src, ins, h):
        mine = src[p.y, h].astype(F32)
        from_up, from_down = (0, 2) if h == 0 else (3, 1)
        return mine + ins[from_up].astype(F32) + ins[from_down].astype(F32)

    square = None
    for h in range(2):
        cols = slice(h * 1024, h * 1024 + 1024)
        m = x_ref[:, cols].astype(F32) + own_sum(part, rs_in, h)
        mid[:, cols] = m
        sq = jnp.sum(m * m, axis=1, keepdims=True)
        square = sq if square is None else square + sq
    inv = lax.rsqrt(square * (1.0 / 2048) + norm_eps)
    for h in range(2):
        cols = slice(h * 1024, h * 1024 + 1024)
        ag[p.y, h] = (mid[:, cols] * inv * gain_ref[:, cols]).astype(BF16)

    def ag_copy(k, d, h, y):
        return to_y(ag.at[d, h], ag.at[d, h], ag_s.at[k], ag_r.at[k], y)

    gathers = (
        ag_copy(0, p.y, 0, up), ag_copy(1, p.y, 1, down), ag_copy(2, p.y, 1, up), ag_copy(3, p.y, 0, down),
        ag_copy(4, down, 0, up), ag_copy(5, up, 1, down),
    )
    for copy in gathers[:4]:
        copy.start()

    def weights_pair(t):
        w.z_b(t)
        if t + 1 < NSETS:
            w.z_b(t + 1)
        w.z_a(t)
        if t + 1 < NSETS:
            w.z_a(t + 1)
        for u in (t, t + 1):
            if u < NSETS:
                w.x1(u)
                w.x2(u)
                w.x3(u)
                w.arrived(u)

    weights_pair(1)
    gathers[0].wait_recv()
    gathers[4].start()
    gathers[1].wait_recv()
    gathers[5].start()
    for t in (3, 5, 7):
        weights_pair(t)
    for copy in gathers[2:]:
        copy.wait_recv()

    rows = [ag[:, h].reshape(256, 1024) for h in range(2)]
    for m in range(2):
        for k in range(3):
            cols = slice(k * 256, k * 256 + 256)
            tile = None
            for h in range(2):
                block = wgu[16 * h:16 * h + 16, :, m, :, cols].reshape(1024, 256)
                o = dot(rows[h], block)
                tile = o if tile is None else tile + o
            pre[:, m * 768 + k * 256:m * 768 + k * 256 + 256] = tile.astype(BF16)

    def halo_copy(k, src, sp):
        return pltpu.make_async_remote_copy(src_ref=src, dst_ref=halo.at[k], send_sem=h_s.at[k], recv_sem=h_r.at[k],
                                            device_id={"sp": sp}, device_id_type=MESH)

    halos = (halo_copy(0, pre.at[240:256, :], sp_next), halo_copy(1, pre.at[0:16, :], sp_prev))
    for copy in halos:
        copy.start()
    for copy in halos:
        copy.wait_recv()
    keep_prev = jnp.where(p.sp == 0, 0.0, 1.0).astype(F32)
    keep_next = jnp.where(p.sp == 63, 0.0, 1.0).astype(F32)
    row = lax.broadcasted_iota(jnp.int32, (256, 256), 0)
    for k in range(3):
        mixed = []
        for m, taps in ((0, cg_ref), (1, cu_ref)):
            cols = slice(m * 768 + k * 256, m * 768 + k * 256 + 256)
            tcols = slice(k * 256, k * 256 + 256)
            now = pre[:, cols].astype(F32)
            before = halo[0, :, cols].astype(F32)[15:16, :] * keep_prev
            after = halo[1, :, cols].astype(F32)[0:1, :] * keep_next
            prev = jnp.where(row == 0, before, pltpu.roll(now, 1, 0))
            nxt = jnp.where(row == 255, after, pltpu.roll(now, 255, 0))
            mixed.append(prev * taps[0:1, tcols] + now * taps[1:2, tcols] + nxt * taps[2:3, tcols])
        gate, upv = mixed
        hid[:, k * 256:k * 256 + 256] = (gate / (1.0 + jnp.exp(-gate)) * upv).astype(BF16)

    for k in range(8):
        block = wd[4 * k:4 * k + 4].reshape(256, 768)
        tile = lax.dot_general(hid[...], block, (((1,), (1,)), ((), ())), preferred_element_type=F32)
        part2[:, k // 4, :, (k % 4) * 256:(k % 4) * 256 + 256] = tile.astype(BF16).reshape(4, 64, 256)

    second = reduce_copies(part2, rs_mid2, rs_in2, rs_s2, rs_r2)
    reduce_first(second)
    g.drain()
    w.drain()
    reduce_second(second, part2, rs_mid2)
    reduce_last(second)
    for h in range(2):
        cols = slice(h * 1024, h * 1024 + 1024)
        out_ref[:, cols] = (mid[:, cols] + own_sum(part2, rs_in2, h)).astype(BF16)
    for copy in (*first, *second, *gathers, *halos):
        copy.wait_send()


def fused(*args):
    vm = pl.BlockSpec(memory_space=pltpu.VMEM)
    hb = pl.BlockSpec(memory_space=pltpu.HBM)
    v, d = pltpu.VMEM, pltpu.SemaphoreType.DMA
    scratch = [
        v((2, NZ, NX, 256, 128), BF16), v((2, NZ, NX, 512, 128), BF16),
        v((32, 2, 2, 32, 768), BF16), v((32, 2, 32, 768), BF16),
        v((256, 2048), BF16), v((256, 2048), BF16),
        v((2048, 256), F32), v((2048, 256), F32), v((2048, 256), BF16),
        v((4, 80, 256), F32), v((2, 144, 256), F32), v((6, 1, 256), F32),
        v((256, 512), BF16), v((4, 2, 64, 1024), BF16), v((4, 64, 1024), BF16), v((4, 64, 1024), BF16),
        v((64, 2048), F32), v((4, 2, 64, 1024), BF16), v((256, 1536), BF16), v((2, 16, 1536), BF16),
        v((256, 768), BF16), v((4, 2, 64, 1024), BF16), v((4, 64, 1024), BF16), v((4, 64, 1024), BF16),
        d((4,)), d((2,)), d((6,)), d((6,)), d((6,)), d((6,)), d((6,)), d((6,)), d((2,)), d((2,)),
        *gather_sems(), *gather_sems(),
    ]
    return pl.pallas_call(
        kernel,
        out_shape=jax.ShapeDtypeStruct((64, 2048), BF16),
        in_specs=[hb, hb, vm, vm, hb, hb, hb, hb, vm, vm, vm, vm],
        out_specs=vm,
        scratch_shapes=scratch,
        compiler_params=pltpu.CompilerParams(
            collective_id=0, has_side_effects=True, vmem_limit_bytes=60 * 1024 * 1024
        ),
        name="layer",
    )(*args)


def on_device(
    x_res, q_a, k_a, v_a, q_b, k_b, v_b, gain_qa, gain_ka, gain_qb, gain_kb,
    w_out_a, w_out_b, gain_mid, w_gate, w_up, conv_gate, conv_up, w_down,
):
    rows = q_a.shape[0]
    positions = lax.axis_index("sp") * rows + lax.iota(jnp.int32, rows)
    qa = prepare(q_a, gain_qa, DHA, positions)
    qb = prepare(q_b, gain_qb, DHB, positions)
    ka = prepare(k_a, gain_ka, DHA, positions)[:, 0]
    kb = prepare(k_b, gain_kb, DHB, positions)[:, 0]
    qa_t = jnp.transpose(qa * BF16(0.125), (1, 2, 0))
    qb_t = jnp.transpose(qb, (1, 2, 0))
    ka2 = jnp.concatenate([ka[:128], ka[128:]], axis=1)
    kva = jnp.concatenate([ka2, v_a[:128].T, v_a[128:].T], axis=0)
    kvb = jnp.concatenate([kb, v_b[:128].T, v_b[128:].T], axis=0)
    wgu = jnp.stack([w_gate, w_up])
    return fused(kva, kvb, qa_t, qb_t, wgu, w_down.T, w_out_a, w_out_b, x_res, gain_mid[None, :], conv_gate, conv_up)


def solution(mesh):
    in_specs = (
        P(("sp", "tp"), None), P("sp", "tp"), P("sp", "tp"), P("sp", "tp"), P("sp", "tp"), P("sp", "tp"), P("sp", "tp"),
        P(), P(), P(), P(), P("tp", None), P("tp", None), P(),
        P("sp", "tp"), P("sp", "tp"), P(None, "tp"), P(None, "tp"), P("tp", "sp"),
    )
    return jax.shard_map(
        on_device, mesh=mesh, in_specs=in_specs, out_specs=P(("sp", "tp"), None), check_vma=False
    )
```

```python
import functools
import math

import jax
import jax.numpy as jnp
import numpy as np
from jax import lax
from jax.experimental import pallas as pl
from jax.experimental.pallas import tpu as pltpu
from jax.sharding import PartitionSpec as P

DHA = 64
DHB = 128
NZ = 8
NX = 4
NY = 4
NSETS = NZ
MESH = pl.DeviceIdType.MESH
F32 = jnp.float32
BF16 = jnp.bfloat16
LOG2E = math.log2(math.e)

norm_eps = 1e-06
rope_theta = 10000.0


def rotary_tables(head_size):
    half = head_size // 2
    quarter = head_size // 4
    inverse = np.power(np.float32(rope_theta), -np.arange(0, half, 2, dtype=np.float32) / np.float32(half)).astype(np.float32)
    lane = np.arange(128)
    per_lane = inverse[lane % quarter]
    sign = np.where(lane % half < quarter, -1.0, 1.0)
    angle_r = (np.arange(256, dtype=np.float32)[:, None] * per_lane[None, :]).astype(np.float64)
    rows = np.concatenate([np.cos(angle_r).reshape(64, 4, 128), (np.sin(angle_r) * sign).reshape(64, 4, 128)], axis=1)
    angle_c = angle_r[:64]
    cols = np.stack([np.cos(angle_c), np.sin(angle_c) * sign])
    return rows.astype(np.float32), cols.astype(np.float32)


class Place:
    def __init__(self):
        self.sp = lax.axis_index("sp")
        self.y = lax.axis_index("tp")
        self.c = self.sp % 2
        self.x = (self.sp // 2) % NX
        self.z = self.sp // (2 * NX)
        self.s = 1 - 2 * self.c

    def at(self, z, x, c):
        return (z * NX + x) * 2 + c

    def zz(self, d):
        return (self.z + d + 2 * NZ) % NZ

    def xx(self, d):
        return (self.x + d + 2 * NX) % NX

    def set_z(self, t, s):
        k = (t + 1) // 2
        sign = 1 - 2 * (t % 2)
        return self.zz(sign * s * k)


class Gather:
    def __init__(self, place, group_a, piece_a, piece_b, sems):
        self.p = place
        self.group_a, self.piece_a, self.piece_b = group_a, piece_a, piece_b
        (self.ax_s, self.ax_r, self.az_s, self.az_r, self.at_s, self.at_r,
         self.bz_s, self.bz_r, self.bx_s, self.bx_r, self.bt_s, self.bt_r) = sems

    def _copy(self, ref, s_sem, r_sem, sp):
        return pltpu.make_async_remote_copy(
            src_ref=ref, dst_ref=ref, send_sem=s_sem, recv_sem=r_sem,
            device_id={"sp": sp}, device_id_type=MESH,
        )

    def c_ax(self, k):
        p = self.p
        src_x = [p.x, p.xx(-p.s), p.x][k]
        to = [p.xx(p.s), p.xx(p.s), p.xx(-p.s)][k]
        return self._copy(self.piece_a(p.z, src_x, p.c), self.ax_s.at[k], self.ax_r.at[k], p.at(p.z, to, p.c))

    def c_az(self, t, to_z, src_z):
        p = self.p
        return self._copy(self.group_a(src_z, p.c), self.az_s.at[t], self.az_r.at[t], p.at(to_z, p.x, p.c))

    def c_at(self, t):
        p = self.p
        return self._copy(self.group_a(p.set_z(t, p.s), p.c), self.at_s.at[t], self.at_r.at[t], p.at(p.z, p.x, 1 - p.c))

    def c_bz(self, t, to_z, src_z):
        p = self.p
        return self._copy(self.piece_b(src_z, p.x, p.c), self.bz_s.at[t], self.bz_r.at[t], p.at(to_z, p.x, p.c))

    def c_bx(self, t, k):
        p = self.p
        src_x = [p.x, p.xx(-p.s), p.x][k]
        to = [p.xx(p.s), p.xx(p.s), p.xx(-p.s)][k]
        return self._copy(self.piece_b(p.set_z(t, p.s), src_x, p.c), self.bx_s.at[t, k], self.bx_r.at[t, k],
                          p.at(p.z, to, p.c))

    def c_bt(self, t, k):
        p = self.p
        src_x = [p.x, p.xx(-p.s), p.xx(p.s), p.xx(-2 * p.s)][k]
        return self._copy(self.piece_b(p.set_z(t, p.s), src_x, p.c), self.bt_s.at[t, k], self.bt_r.at[t, k],
                          p.at(p.z, p.x, 1 - p.c))

    def start_b(self):
        p = self.p
        self.c_bz(1, p.zz(p.s), p.z).start()
        self.c_bz(2, p.zz(-p.s), p.z).start()
        self.c_bx(0, 0).start()
        self.c_bx(0, 2).start()
        self.c_bt(0, 0).start()

    def start_a(self):
        self.c_ax(0).start()
        self.c_ax(2).start()

    def x_a(self):
        p = self.p
        self.c_ax(0).wait_recv()
        self.c_ax(1).start()
        self.c_ax(2).wait_recv()
        self.c_ax(1).wait_recv()
        self.c_az(1, p.zz(p.s), p.z).start()
        self.c_az(2, p.zz(-p.s), p.z).start()
        self.c_at(0).start()

    def _hop(self, t, copy):
        p = self.p
        sign = (2 * (t % 2) - 1) * p.s
        copy(t, p.z, p.set_z(t, p.s)).wait_recv()

        @pl.when(t <= NSETS - 3)
        def _():
            copy(t + 2, p.zz(sign), p.set_z(t, p.s)).start()

    def z_b(self, t):
        self._hop(t, self.c_bz)
        self.c_bx(t, 0).start()
        self.c_bx(t, 2).start()
        self.c_bt(t, 0).start()

    def z_a(self, t):
        self._hop(t, self.c_az)
        self.c_at(t).start()

    def x1(self, t):
        self.c_bx(t, 0).wait_recv()
        self.c_bx(t, 1).start()
        self.c_bt(t, 1).start()

    def x2(self, t):
        self.c_bx(t, 2).wait_recv()
        self.c_bt(t, 2).start()

    def x3(self, t):
        self.c_bx(t, 1).wait_recv()
        self.c_bt(t, 3).start()

    def arrived(self, t):
        self.c_at(t).wait_recv()
        for k in range(4):
            self.c_bt(t, k).wait_recv()

    def drain(self):
        p = self.p
        for k in range(3):
            self.c_ax(k).wait_send()

        @pl.loop(0, NSETS)
        def _(t):
            self.c_at(t).wait_send()
            for k in range(3):
                self.c_bx(t, k).wait_send()
            for k in range(4):
                self.c_bt(t, k).wait_send()

            @pl.when(t >= 1)
            def _():
                self.c_az(t, p.z, p.z).wait_send()
                self.c_bz(t, p.z, p.z).wait_send()


def gather_sems():
    d = pltpu.SemaphoreType.DMA
    return [d((3,)), d((3,)), d((8,)), d((8,)), d((8,)), d((8,)),
            d((8,)), d((8,)), d((8, 3)), d((8, 3)), d((8, 4)), d((8, 4))]


def dot(a, b):
    return jnp.dot(a, b, preferred_element_type=F32)


def kernel(q_a, k_a, v_a, q_b, k_b, v_b, ra_h, rb_h, col_a, col_b, g_qa, g_ka, g_qb, g_kb, wg_h, wu_h, wd_h, woa_h, wob_h, x_ref, gain_ref, cg_ref, cu_ref, out_ref,
           qa_in, ka_in, va_in, qb_in, kb_in, vb_in, ra, rb, qa_ref, qb_ref, ba, bb, wa, wb, woa, wob, s_a, s_b, p_ref, acc_a, acc_b, mx,
           attn, part, rs_mid, rs_in, mid, ag, pre, halo, hid, part2, rs_mid2, rs_in2,
           in_sem, loc, wo_sem, rs_s, rs_r, rs_s2, rs_r2, ag_s, ag_r, h_s, h_r, *sems):
    p = Place()
    n = len(sems) // 2

    barrier = pltpu.get_barrier_semaphore()
    up, down = (p.y + 1) % NY, (p.y + NY - 1) % NY
    opp = (p.y + 2) % NY
    sp_next, sp_prev = (p.sp + 1) % 64, (p.sp + 63) % 64
    pairs = ((k_a, ka_in), (v_a, va_in), (k_b, kb_in), (v_b, vb_in), (ra_h.at[p.sp], ra), (rb_h.at[p.sp], rb),
             (q_a, qa_in), (q_b, qb_in))
    inputs = [pltpu.make_async_copy(src, dst, in_sem.at[i]) for i, (src, dst) in enumerate(pairs)]
    for copy in inputs:
        copy.start()
    zx = p.z * NX + p.x
    own_g = pltpu.make_async_copy(wg_h, wa.at[zx, p.c, :, pl.ds(0, 768)], loc.at[0])
    own_ua = pltpu.make_async_copy(wu_h.at[:, pl.ds(0, 384)], wa.at[zx, p.c, :, pl.ds(768, 384)], loc.at[1])
    own_ub = pltpu.make_async_copy(wu_h.at[:, pl.ds(384, 384)], wb.at[zx, p.c, :, pl.ds(0, 384)], loc.at[2])
    own_d = pltpu.make_async_copy(wd_h, wb.at[zx, p.c, :, pl.ds(384, 768)], loc.at[3])
    own_oa = pltpu.make_async_copy(woa_h, woa, wo_sem.at[0])
    own_ob = pltpu.make_async_copy(wob_h, wob, wo_sem.at[1])
    for copy in (own_g, own_ua, own_ub, own_d, own_oa, own_ob):
        copy.start()
    greeted = [p.at(p.zz(1), p.x, p.c), p.at(p.zz(-1), p.x, p.c), p.at(p.z, p.xx(1), p.c), p.at(p.z, p.xx(-1), p.c),
               p.at(p.z, p.x, 1 - p.c), sp_next, sp_prev]
    for sp in greeted:
        pl.semaphore_signal(barrier, inc=1, device_id={"sp": sp}, device_id_type=MESH)
    for y in (up, down):
        pl.semaphore_signal(barrier, inc=1, device_id={"tp": y}, device_id_type=MESH)

    lane = lax.broadcasted_iota(jnp.int32, (64, 128), 1)
    first_head = lane < 64

    def normed_a(v, gain):
        sq = v * v
        left = jnp.sum(jnp.where(first_head, sq, 0.0), axis=1, keepdims=True)
        right = jnp.sum(jnp.where(first_head, 0.0, sq), axis=1, keepdims=True)
        inv = lax.rsqrt(jnp.where(first_head, left, right) * (1.0 / DHA) + norm_eps)
        gains = jnp.concatenate([gain[...], gain[...]], axis=1)
        return v * inv * gains

    def normed_b(v, gain):
        inv = lax.rsqrt(jnp.sum(v * v, axis=1, keepdims=True) * (1.0 / DHB) + norm_eps)
        return v * inv * gain[...]

    def turned(v, quarter, cos, sin):
        other = jnp.where(lane % (2 * quarter) < quarter, pltpu.roll(v, 128 - quarter, 1), pltpu.roll(v, quarter, 1))
        return v * cos + other * sin

    def turned_a(v, left, right):
        row_lane = lane % 64 < 32

        def table(k):
            row = jnp.where(first_head, ra[4 * k + left:4 * k + left + 1, :], ra[4 * k + right:4 * k + right + 1, :])
            return jnp.where(row_lane, row, col_a[k])

        return turned(v, 16, table(0), table(1))

    def turned_b(v, block):
        def table(k):
            return jnp.where(first_head, rb[4 * k + block:4 * k + block + 1, :], col_b[k])

        return turned(v, 32, table(0), table(1))

    for copy in inputs[:6]:
        copy.wait()
    slot_a, slot_b = ba.at[p.c, p.z, p.x], bb.at[p.c, p.z, p.x]
    ka = ka_in[...].astype(F32).T
    for k in range(2):
        v = jnp.concatenate([ka[64 * k:64 * k + 64, :], ka[128 + 64 * k:192 + 64 * k, :]], axis=1)
        slot_a[64 * k:64 * k + 64, :] = turned_a(normed_a(v, g_ka), k, k + 2).astype(BF16)
    slot_a[128:192, :] = va_in[:, 0:128]
    slot_a[192:256, :] = va_in[:, 128:256]
    for k in range(4):
        v = kb_in[64 * k:64 * k + 64, :].astype(F32)
        slot_b[64 * k:64 * k + 64, :] = turned_b(normed_b(v, g_kb), k).astype(BF16)
    vt = vb_in[...].astype(F32).T.astype(BF16)
    slot_b[256:384, :] = vt[:, 0:128]
    slot_b[384:512, :] = vt[:, 128:256]
    pl.semaphore_wait(barrier, 9)

    g = Gather(p, lambda z, c: ba.at[c, z], lambda z, x, c: ba.at[c, z, x], lambda z, x, c: bb.at[c, z, x], sems[:n])
    w = Gather(p, lambda z, c: wa.at[pl.ds(z * NX, NX), c], lambda z, x, c: wa.at[z * NX + x, c],
               lambda z, x, c: wb.at[z * NX + x, c], sems[n:])

    g.start_a()
    g.start_b()
    inputs[6].wait()
    inputs[7].wait()
    for h in range(2):
        blocks = []
        for k in range(4):
            v = qa_in[64 * k:64 * k + 64, 128 * h:128 * h + 128].astype(F32)
            blocks.append(turned_a(normed_a(v, g_qa), k, k) * 0.125)
        qt = jnp.concatenate(blocks, axis=0).T.astype(BF16)
        qa_ref[2 * h] = qt[0:64, :]
        qa_ref[2 * h + 1] = qt[64:128, :]
    for h in range(2):
        blocks = []
        for k in range(4):
            v = qb_in[64 * k:64 * k + 64, 128 * h:128 * h + 128].astype(F32)
            blocks.append(turned_b(normed_b(v, g_qb), k))
        qb_ref[h] = jnp.concatenate(blocks, axis=0).T.astype(BF16)
    acc_a[...] = jnp.zeros_like(acc_a)
    acc_b[...] = jnp.zeros_like(acc_b)
    mx[...] = jnp.full_like(mx, -1e30)
    g.x_a()
    for copy in (own_g, own_ua, own_ub, own_d):
        copy.wait()
    g.x1(0)
    g.x2(0)
    g.z_b(1)
    g.z_b(2)

    zeros64 = jnp.zeros((64, 256), BF16)

    def scores(tile, buf, parts):
        top = None
        if tile < 4:
            q = qa_ref[tile]
            both = (jnp.concatenate([q, zeros64], axis=0), jnp.concatenate([zeros64, q], axis=0))
            for i, (cc, z) in enumerate(parts):
                keys = ba[cc, z, :, 0:128, :].reshape(512, 128)
                for h in range(2):
                    sc = dot(keys, both[h])
                    buf[pl.ds((i * 2 + h) * 512, 512), :] = sc
                    m8 = jnp.max(sc.reshape(64, 8, 256), axis=0)
                    top = m8 if top is None else jnp.maximum(top, m8)
        else:
            q = qb_ref[tile - 4]
            for i, (cc, z) in enumerate(parts):
                for h in range(2):
                    keys = bb[cc, z, 2 * h:2 * h + 2, 0:256, :].reshape(512, 128)
                    sc = dot(keys, q)
                    buf[pl.ds((i * 2 + h) * 512, 512), :] = sc
                    m8 = jnp.max(sc.reshape(64, 8, 256), axis=0)
                    top = m8 if top is None else jnp.maximum(top, m8)
        return jnp.max(top, axis=0, keepdims=True)

    def weigh(tile, buf, top, parts):
        scale = LOG2E if tile < 4 else LOG2E * DHB ** -0.5
        old = mx[tile]
        new = jnp.maximum(old, top * scale)
        mx[tile] = new
        factor = jnp.exp2(old - new)
        total = None
        for i, (cc, z) in enumerate(parts):
            for h in range(2):
                rows = pl.ds((i * 2 + h) * 512, 512)
                p_ref[rows, :] = jnp.exp2(buf[rows, :] * scale - new).astype(BF16)
                if tile < 4:
                    vt = jnp.concatenate([ba[cc, z, x, 128 + 64 * h:192 + 64 * h, :] for x in range(4)], axis=1)
                else:
                    vt = jnp.concatenate(
                        [bb[cc, z, x, 256 + 128 * e:384 + 128 * e, :] for x in (2 * h, 2 * h + 1) for e in range(2)], axis=1)
                vt = jnp.concatenate([vt, jnp.ones((16, 512), BF16)], axis=0)
                o = dot(vt, p_ref[rows, :])
                total = o if total is None else total + o
        if tile < 4:
            acc_a[tile] = acc_a[tile] * factor + total
        else:
            acc_b[tile - 4] = acc_b[tile - 4] * factor + total

    @pl.loop(1, NSETS + 1)
    def _(t):
        odd = t % 2 == 1
        parts = ((p.c, p.set_z(t - 1, p.s)), (1 - p.c, p.set_z(t - 1, -p.s)))
        g.x3(t - 1)
        g.arrived(t - 1)

        @pl.when(odd)
        def _():
            g.x1(t)
            g.x2(t)

        bufs = (s_a, s_b)
        top = scores(0, bufs[0], parts)
        for i in range(6):
            following = scores(i + 1, bufs[(i + 1) % 2], parts) if i < 5 else None
            weigh(i, bufs[i % 2], top, parts)
            top = following
            if i == 1:
                @pl.when(odd)
                def _():
                    g.z_a(t)

                    @pl.when(t + 1 < NSETS)
                    def _():
                        g.z_a(t + 1)

                @pl.when(t == 4)
                def _():
                    w.start_a()
                    w.start_b()
            if i == 3:
                @pl.when(jnp.logical_and(odd, t + 1 < NSETS))
                def _():
                    g.x1(t + 1)
                    g.x2(t + 1)

                @pl.when(t == 6)
                def _():
                    w.x_a()
                    w.x1(0)
            if i == 5:
                @pl.when(jnp.logical_and(odd, t + 2 < NSETS))
                def _():
                    g.z_b(t + 2)

                    @pl.when(t + 3 < NSETS)
                    def _():
                        g.z_b(t + 3)

    def w_b(t):
        for u in (t, t + 1):
            if u < NSETS:
                w.z_b(u)

    def w_a(t):
        for u in (t, t + 1):
            if u < NSETS:
                w.z_a(u)

    def w_x(t):
        for u in (t, t + 1):
            if u < NSETS:
                w.x1(u)


    o_a = [acc_a[h, 0:64, :] / acc_a[h, 64:65, :] for h in range(4)]
    attn[:, 0:256] = jnp.concatenate(o_a, axis=0).T.astype(BF16)
    o_b = [acc_b[h, 0:128, :] / acc_b[h, 128:129, :] for h in range(2)]
    attn[:, 256:512] = jnp.concatenate(o_b, axis=0).T.astype(BF16)
    own_oa.wait()
    own_ob.wait()
    for k in range(8):
        cols = slice(k * 256, k * 256 + 256)
        tile = dot(attn[:, 0:256], woa[:, cols]) + dot(attn[:, 256:512], wob[:, cols])
        part[:, k // 4, :, (k % 4) * 256:(k % 4) * 256 + 256] = tile.astype(BF16).reshape(4, 64, 256)

    def to_y(src, dst, s_sem, r_sem, y):
        return pltpu.make_async_remote_copy(src_ref=src, dst_ref=dst, send_sem=s_sem, recv_sem=r_sem,
                                            device_id={"tp": y}, device_id_type=MESH)

    def reduce_copies(src, mids, ins, ss, rr):
        return (
            to_y(src.at[opp, 0], mids.at[0], ss.at[0], rr.at[0], up),
            to_y(src.at[opp, 1], mids.at[1], ss.at[1], rr.at[1], down),
            to_y(src.at[down, 0], ins.at[0], ss.at[2], rr.at[2], down),
            to_y(src.at[up, 1], ins.at[1], ss.at[3], rr.at[3], up),
            to_y(mids.at[2], ins.at[2], ss.at[4], rr.at[4], up),
            to_y(mids.at[3], ins.at[3], ss.at[5], rr.at[5], down),
        )

    def reduce_first(copies):
        for copy in copies[:4]:
            copy.start()

    def reduce_second(copies, src, mids):
        copies[0].wait_recv()
        mids[2] = (src[up, 0].astype(F32) + mids[0].astype(F32)).astype(BF16)
        copies[1].wait_recv()
        mids[3] = (src[down, 1].astype(F32) + mids[1].astype(F32)).astype(BF16)
        copies[4].start()
        copies[5].start()

    def reduce_last(copies):
        for copy in copies[2:]:
            copy.wait_recv()

    first = reduce_copies(part, rs_mid, rs_in, rs_s, rs_r)
    reduce_first(first)
    w_b(1)
    w_a(1)
    w_x(1)
    reduce_second(first, part, rs_mid)
    w_b(3)
    reduce_last(first)

    def own_sum(src, ins, h):
        mine = src[p.y, h].astype(F32)
        from_up, from_down = (0, 2) if h == 0 else (3, 1)
        return mine + ins[from_up].astype(F32) + ins[from_down].astype(F32)

    square = None
    for h in range(2):
        cols = slice(h * 1024, h * 1024 + 1024)
        m = x_ref[:, cols].astype(F32) + own_sum(part, rs_in, h)
        mid[:, cols] = m
        sq = jnp.sum(m * m, axis=1, keepdims=True)
        square = sq if square is None else square + sq
    inv = lax.rsqrt(square * (1.0 / 2048) + norm_eps)
    for h in range(2):
        cols = slice(h * 1024, h * 1024 + 1024)
        ag[p.y, h] = (mid[:, cols] * inv * gain_ref[:, cols]).astype(BF16)

    def ag_copy(k, d, h, y):
        return to_y(ag.at[d, h], ag.at[d, h], ag_s.at[k], ag_r.at[k], y)

    gathers = (
        ag_copy(0, p.y, 0, up), ag_copy(1, p.y, 1, down), ag_copy(2, p.y, 1, up), ag_copy(3, p.y, 0, down),
        ag_copy(4, down, 0, up), ag_copy(5, up, 1, down),
    )
    for copy in gathers[:4]:
        copy.start()

    w_a(3)
    w_x(3)
    gathers[0].wait_recv()
    gathers[4].start()
    gathers[1].wait_recv()
    gathers[5].start()
    for t in (5, 7):
        w_b(t)
        w_a(t)
        w_x(t)

    @pl.loop(0, NSETS)
    def _(t):
        w.x2(t)
        w.x3(t)

    @pl.loop(0, NSETS)
    def _(t):
        w.arrived(t)

    for copy in gathers[2:]:
        copy.wait_recv()

    rows = [ag[:, h].reshape(256, 1024) for h in range(2)]
    for m in range(2):
        for k in range(3):
            cols = slice(k * 256, k * 256 + 256)
            tile = None
            for h in range(2):
                half = slice(16 * h, 16 * h + 16)
                if m == 0:
                    block = wa[half, :, :, cols]
                elif k == 0:
                    block = wa[half, :, :, 768:1024]
                elif k == 1:
                    block = jnp.concatenate([wa[half, :, :, 1024:1152], wb[half, :, :, 0:128]], axis=-1)
                else:
                    block = wb[half, :, :, 128:384]
                block = block.reshape(1024, 256)
                o = dot(rows[h], block)
                tile = o if tile is None else tile + o
            pre[:, m * 768 + k * 256:m * 768 + k * 256 + 256] = tile.astype(BF16)

    def halo_copy(k, src, sp):
        return pltpu.make_async_remote_copy(src_ref=src, dst_ref=halo.at[k], send_sem=h_s.at[k], recv_sem=h_r.at[k],
                                            device_id={"sp": sp}, device_id_type=MESH)

    halos = (halo_copy(0, pre.at[240:256, :], sp_next), halo_copy(1, pre.at[0:16, :], sp_prev))
    for copy in halos:
        copy.start()
    for copy in halos:
        copy.wait_recv()
    keep_prev = jnp.where(p.sp == 0, 0.0, 1.0).astype(F32)
    keep_next = jnp.where(p.sp == 63, 0.0, 1.0).astype(F32)
    row = lax.broadcasted_iota(jnp.int32, (256, 256), 0)
    for k in range(3):
        mixed = []
        for m, taps in ((0, cg_ref), (1, cu_ref)):
            cols = slice(m * 768 + k * 256, m * 768 + k * 256 + 256)
            tcols = slice(k * 256, k * 256 + 256)
            now = pre[:, cols].astype(F32)
            before = halo[0, :, cols].astype(F32)[15:16, :] * keep_prev
            after = halo[1, :, cols].astype(F32)[0:1, :] * keep_next
            prev = jnp.where(row == 0, before, pltpu.roll(now, 1, 0))
            nxt = jnp.where(row == 255, after, pltpu.roll(now, 255, 0))
            mixed.append(prev * taps[0:1, tcols] + now * taps[1:2, tcols] + nxt * taps[2:3, tcols])
        gate, upv = mixed
        hid[:, k * 256:k * 256 + 256] = (gate / (1.0 + jnp.exp(-gate)) * upv).astype(BF16)

    for k in range(8):
        block = wb[4 * k:4 * k + 4, :, :, 384:1152].reshape(256, 768)
        tile = lax.dot_general(hid[...], block, (((1,), (1,)), ((), ())), preferred_element_type=F32)
        part2[:, k // 4, :, (k % 4) * 256:(k % 4) * 256 + 256] = tile.astype(BF16).reshape(4, 64, 256)

    second = reduce_copies(part2, rs_mid2, rs_in2, rs_s2, rs_r2)
    reduce_first(second)
    g.drain()
    w.drain()
    reduce_second(second, part2, rs_mid2)
    reduce_last(second)
    for h in range(2):
        cols = slice(h * 1024, h * 1024 + 1024)
        out_ref[:, cols] = (mid[:, cols] + own_sum(part2, rs_in2, h)).astype(BF16)
    for copy in (*first, *second, *gathers, *halos):
        copy.wait_send()


def fused(*args):
    vm = pl.BlockSpec(memory_space=pltpu.VMEM)
    hb = pl.BlockSpec(memory_space=pltpu.HBM)
    v, d = pltpu.VMEM, pltpu.SemaphoreType.DMA
    scratch = [
        v((256, 256), BF16), v((64, 256), BF16), v((64, 256), BF16), v((256, 256), BF16), v((256, 128), BF16),
        v((256, 128), BF16), v((8, 128), F32), v((8, 128), F32),
        v((4, 64, 256), BF16), v((2, 128, 256), BF16),
        v((2, NZ, NX, 256, 128), BF16), v((2, NZ, NX, 512, 128), BF16),
        v((32, 2, 32, 1152), BF16), v((32, 2, 32, 1152), BF16),
        v((256, 2048), BF16), v((256, 2048), BF16),
        v((2048, 256), F32), v((2048, 256), F32), v((2048, 256), BF16),
        v((4, 80, 256), F32), v((2, 144, 256), F32), v((6, 1, 256), F32),
        v((256, 512), BF16), v((4, 2, 64, 1024), BF16), v((4, 64, 1024), BF16), v((4, 64, 1024), BF16),
        v((64, 2048), F32), v((4, 2, 64, 1024), BF16), v((256, 1536), BF16), v((2, 16, 1536), BF16),
        v((256, 768), BF16), v((4, 2, 64, 1024), BF16), v((4, 64, 1024), BF16), v((4, 64, 1024), BF16),
        d((8,)), d((4,)), d((2,)), d((6,)), d((6,)), d((6,)), d((6,)), d((6,)), d((6,)), d((2,)), d((2,)),
        *gather_sems(), *gather_sems(),
    ]
    return pl.pallas_call(
        kernel,
        out_shape=jax.ShapeDtypeStruct((64, 2048), BF16),
        in_specs=[hb] * 8 + [vm] * 6 + [hb] * 5 + [vm] * 4,
        out_specs=vm,
        scratch_shapes=scratch,
        compiler_params=pltpu.CompilerParams(
            collective_id=0, has_side_effects=True, vmem_limit_bytes=60 * 1024 * 1024
        ),
        name="layer",
    )(*args)


def on_device(
    x_res, q_a, k_a, v_a, q_b, k_b, v_b, gain_qa, gain_ka, gain_qb, gain_kb,
    w_out_a, w_out_b, gain_mid, w_gate, w_up, conv_gate, conv_up, w_down,
):
    rows_a, cols_a = rotary_tables(DHA)
    rows_b, cols_b = rotary_tables(DHB)
    return fused(
        q_a, k_a.T, v_a.T, q_b, k_b, v_b, rows_a, rows_b, cols_a, cols_b,
        gain_qa[None, :], gain_ka[None, :], gain_qb[None, :], gain_kb[None, :],
        w_gate, w_up, w_down.T, w_out_a, w_out_b, x_res, gain_mid[None, :], conv_gate, conv_up,
    )


def solution(mesh):
    in_specs = (
        P(("sp", "tp"), None), P("sp", "tp"), P("sp", "tp"), P("sp", "tp"), P("sp", "tp"), P("sp", "tp"), P("sp", "tp"),
        P(), P(), P(), P(), P("tp", None), P("tp", None), P(),
        P("sp", "tp"), P("sp", "tp"), P(None, "tp"), P(None, "tp"), P("tp", "sp"),
    )
    return jax.shard_map(
        on_device, mesh=mesh, in_specs=in_specs, out_specs=P(("sp", "tp"), None), check_vma=False
    )
```

```python
import functools
import math

import jax
import jax.numpy as jnp
import numpy as np
from jax import lax
from jax.experimental import pallas as pl
from jax.experimental.pallas import tpu as pltpu
from jax.sharding import PartitionSpec as P

DHA = 64
DHB = 128
NZ = 8
NX = 4
NY = 4
NSETS = NZ
W_START = 1
W_FIRST = 3
MESH = pl.DeviceIdType.MESH
F32 = jnp.float32
BF16 = jnp.bfloat16
LOG2E = math.log2(math.e)

norm_eps = 1e-06
rope_theta = 10000.0


def rotary_tables(head_size):
    half = head_size // 2
    quarter = head_size // 4
    inverse = np.power(np.float32(rope_theta), -np.arange(0, half, 2, dtype=np.float32) / np.float32(half)).astype(np.float32)
    lane = np.arange(128)
    per_lane = inverse[lane % quarter]
    sign = np.where(lane % half < quarter, -1.0, 1.0)
    angle_r = (np.arange(256, dtype=np.float32)[:, None] * per_lane[None, :]).astype(np.float64)
    rows = np.concatenate([np.cos(angle_r).reshape(64, 4, 128), (np.sin(angle_r) * sign).reshape(64, 4, 128)], axis=1)
    angle_c = angle_r[:64]
    cols = np.stack([np.cos(angle_c), np.sin(angle_c) * sign])
    return rows.astype(np.float32), cols.astype(np.float32)


class Place:
    def __init__(self):
        self.sp = lax.axis_index("sp")
        self.y = lax.axis_index("tp")
        self.c = self.sp % 2
        self.x = (self.sp // 2) % NX
        self.z = self.sp // (2 * NX)
        self.s = 1 - 2 * self.c

    def at(self, z, x, c):
        return (z * NX + x) * 2 + c

    def zz(self, d):
        return (self.z + d + 2 * NZ) % NZ

    def xx(self, d):
        return (self.x + d + 2 * NX) % NX

    def set_z(self, t, s):
        k = (t + 1) // 2
        sign = 1 - 2 * (t % 2)
        return self.zz(sign * s * k)


class Gather:
    def __init__(self, place, group_a, piece_a, piece_b, sems):
        self.p = place
        self.group_a, self.piece_a, self.piece_b = group_a, piece_a, piece_b
        (self.ax_s, self.ax_r, self.az_s, self.az_r, self.at_s, self.at_r,
         self.bz_s, self.bz_r, self.bx_s, self.bx_r, self.bt_s, self.bt_r) = sems

    def _copy(self, ref, s_sem, r_sem, sp):
        return pltpu.make_async_remote_copy(
            src_ref=ref, dst_ref=ref, send_sem=s_sem, recv_sem=r_sem,
            device_id={"sp": sp}, device_id_type=MESH,
        )

    def c_ax(self, k):
        p = self.p
        src_x = [p.x, p.xx(-p.s), p.x][k]
        to = [p.xx(p.s), p.xx(p.s), p.xx(-p.s)][k]
        return self._copy(self.piece_a(p.z, src_x, p.c), self.ax_s.at[k], self.ax_r.at[k], p.at(p.z, to, p.c))

    def c_az(self, t, to_z, src_z):
        p = self.p
        return self._copy(self.group_a(src_z, p.c), self.az_s.at[t], self.az_r.at[t], p.at(to_z, p.x, p.c))

    def c_at(self, t):
        p = self.p
        return self._copy(self.group_a(p.set_z(t, p.s), p.c), self.at_s.at[t], self.at_r.at[t], p.at(p.z, p.x, 1 - p.c))

    def c_bz(self, t, to_z, src_z):
        p = self.p
        return self._copy(self.piece_b(src_z, p.x, p.c), self.bz_s.at[t], self.bz_r.at[t], p.at(to_z, p.x, p.c))

    def c_bx(self, t, k):
        p = self.p
        src_x = [p.x, p.xx(-p.s), p.x][k]
        to = [p.xx(p.s), p.xx(p.s), p.xx(-p.s)][k]
        return self._copy(self.piece_b(p.set_z(t, p.s), src_x, p.c), self.bx_s.at[t, k], self.bx_r.at[t, k],
                          p.at(p.z, to, p.c))

    def c_bt(self, t, k):
        p = self.p
        src_x = [p.x, p.xx(-p.s), p.xx(p.s), p.xx(-2 * p.s)][k]
        return self._copy(self.piece_b(p.set_z(t, p.s), src_x, p.c), self.bt_s.at[t, k], self.bt_r.at[t, k],
                          p.at(p.z, p.x, 1 - p.c))

    def start_b(self):
        p = self.p
        self.c_bz(1, p.zz(p.s), p.z).start()
        self.c_bz(2, p.zz(-p.s), p.z).start()
        self.c_bx(0, 0).start()
        self.c_bx(0, 2).start()
        self.c_bt(0, 0).start()

    def start_a(self):
        self.c_ax(0).start()
        self.c_ax(2).start()

    def x_a1(self):
        self.c_ax(0).wait_recv()
        self.c_ax(1).start()

    def x_a2(self):
        p = self.p
        self.c_ax(2).wait_recv()
        self.c_ax(1).wait_recv()
        self.c_az(1, p.zz(p.s), p.z).start()
        self.c_az(2, p.zz(-p.s), p.z).start()
        self.c_at(0).start()

    def _hop(self, t, copy):
        p = self.p
        sign = (2 * (t % 2) - 1) * p.s
        copy(t, p.z, p.set_z(t, p.s)).wait_recv()

        @pl.when(t <= NSETS - 3)
        def _():
            copy(t + 2, p.zz(sign), p.set_z(t, p.s)).start()

    def z_b(self, t):
        self._hop(t, self.c_bz)
        self.c_bx(t, 0).start()
        self.c_bx(t, 2).start()
        self.c_bt(t, 0).start()

    def z_a(self, t):
        self._hop(t, self.c_az)
        self.c_at(t).start()

    def x1(self, t):
        self.c_bx(t, 0).wait_recv()
        self.c_bx(t, 1).start()
        self.c_bt(t, 1).start()

    def x2(self, t):
        self.c_bx(t, 2).wait_recv()
        self.c_bt(t, 2).start()

    def x3(self, t):
        self.c_bx(t, 1).wait_recv()
        self.c_bt(t, 3).start()

    def arrived(self, t):
        self.c_at(t).wait_recv()
        for k in range(4):
            self.c_bt(t, k).wait_recv()

    def drain(self):
        p = self.p
        for k in range(3):
            self.c_ax(k).wait_send()

        @pl.loop(0, NSETS)
        def _(t):
            self.c_at(t).wait_send()
            for k in range(3):
                self.c_bx(t, k).wait_send()
            for k in range(4):
                self.c_bt(t, k).wait_send()

            @pl.when(t >= 1)
            def _():
                self.c_az(t, p.z, p.z).wait_send()
                self.c_bz(t, p.z, p.z).wait_send()


def gather_sems():
    d = pltpu.SemaphoreType.DMA
    return [d((3,)), d((3,)), d((8,)), d((8,)), d((8,)), d((8,)),
            d((8,)), d((8,)), d((8, 3)), d((8, 3)), d((8, 4)), d((8, 4))]


def dot(a, b):
    return jnp.dot(a, b, preferred_element_type=F32)


def kernel(q_a, k_a, v_a, q_b, k_b, v_b, ra_h, rb_h, col_a, col_b, g_qa, g_ka, g_qb, g_kb, wg_h, wu_h, wd_h, woa_h, wob_h, x_ref, gain_ref, cg_ref, cu_ref, out_ref,
           qa_in, ka_in, va_in, qb_in, kb_in, vb_in, ra, rb, qa_ref, qb_ref, ba, bb, wa, wb, woa, wob, s_a, s_b, p_ref, acc_a, acc_b, mx,
           attn, part, rs_mid, rs_in, mid, ag, pre, edge, hid, part2, rs_mid2, rs_in2,
           in_sem, loc, wo_sem, rs_s, rs_r, rs_s2, rs_r2, ag_s, ag_r, h_s, h_r, *sems):
    p = Place()
    n = len(sems) // 2

    barrier = pltpu.get_barrier_semaphore()
    up, down = (p.y + 1) % NY, (p.y + NY - 1) % NY
    opp = (p.y + 2) % NY
    sp_next, sp_prev = (p.sp + 1) % 64, (p.sp + 63) % 64
    pairs = ((k_a, ka_in), (v_a, va_in), (k_b, kb_in), (v_b, vb_in), (ra_h.at[p.sp], ra), (rb_h.at[p.sp], rb),
             (q_a, qa_in), (q_b, qb_in))
    inputs = [pltpu.make_async_copy(src, dst, in_sem.at[i]) for i, (src, dst) in enumerate(pairs)]
    for copy in inputs:
        copy.start()
    zx = p.z * NX + p.x
    own_g = pltpu.make_async_copy(wg_h, wa.at[zx, p.c, :, pl.ds(0, 768)], loc.at[0])
    own_ua = pltpu.make_async_copy(wu_h.at[:, pl.ds(0, 384)], wa.at[zx, p.c, :, pl.ds(768, 384)], loc.at[1])
    own_ub = pltpu.make_async_copy(wu_h.at[:, pl.ds(384, 384)], wb.at[zx, p.c, :, pl.ds(0, 384)], loc.at[2])
    own_d = pltpu.make_async_copy(wd_h, wb.at[zx, p.c, :, pl.ds(384, 768)], loc.at[3])
    own_oa = pltpu.make_async_copy(woa_h, woa, wo_sem.at[0])
    own_ob = pltpu.make_async_copy(wob_h, wob, wo_sem.at[1])
    for copy in (own_g, own_ua, own_ub, own_d, own_oa, own_ob):
        copy.start()
    greeted = [p.at(p.zz(1), p.x, p.c), p.at(p.zz(-1), p.x, p.c), p.at(p.z, p.xx(1), p.c), p.at(p.z, p.xx(-1), p.c),
               p.at(p.z, p.x, 1 - p.c), sp_next, sp_prev]
    for sp in greeted:
        pl.semaphore_signal(barrier, inc=1, device_id={"sp": sp}, device_id_type=MESH)
    for y in (up, down):
        pl.semaphore_signal(barrier, inc=1, device_id={"tp": y}, device_id_type=MESH)
    for sp in (sp_next, sp_prev):
        for y in (up, down, opp):
            pl.semaphore_signal(barrier, inc=1, device_id={"sp": sp, "tp": y}, device_id_type=MESH)

    lane = lax.broadcasted_iota(jnp.int32, (64, 128), 1)
    first_head = lane < 64

    def normed_a(v, gain):
        sq = v * v
        left = jnp.sum(jnp.where(first_head, sq, 0.0), axis=1, keepdims=True)
        right = jnp.sum(jnp.where(first_head, 0.0, sq), axis=1, keepdims=True)
        inv = lax.rsqrt(jnp.where(first_head, left, right) * (1.0 / DHA) + norm_eps)
        gains = jnp.concatenate([gain[...], gain[...]], axis=1)
        return v * inv * gains

    def normed_b(v, gain):
        inv = lax.rsqrt(jnp.sum(v * v, axis=1, keepdims=True) * (1.0 / DHB) + norm_eps)
        return v * inv * gain[...]

    def turned(v, quarter, cos, sin):
        other = jnp.where(lane % (2 * quarter) < quarter, pltpu.roll(v, 128 - quarter, 1), pltpu.roll(v, quarter, 1))
        return v * cos + other * sin

    def turned_a(v, left, right):
        row_lane = lane % 64 < 32

        def table(k):
            row = jnp.where(first_head, ra[4 * k + left:4 * k + left + 1, :], ra[4 * k + right:4 * k + right + 1, :])
            return jnp.where(row_lane, row, col_a[k])

        return turned(v, 16, table(0), table(1))

    def turned_b(v, block):
        def table(k):
            return jnp.where(first_head, rb[4 * k + block:4 * k + block + 1, :], col_b[k])

        return turned(v, 32, table(0), table(1))

    for copy in inputs[:6]:
        copy.wait()
    slot_a, slot_b = ba.at[p.c, p.z, p.x], bb.at[p.c, p.z, p.x]
    ka = ka_in[...].astype(F32).T
    for k in range(2):
        v = jnp.concatenate([ka[64 * k:64 * k + 64, :], ka[128 + 64 * k:192 + 64 * k, :]], axis=1)
        slot_a[64 * k:64 * k + 64, :] = turned_a(normed_a(v, g_ka), k, k + 2).astype(BF16)
    slot_a[128:192, :] = va_in[:, 0:128]
    slot_a[192:256, :] = va_in[:, 128:256]
    for k in range(4):
        v = kb_in[64 * k:64 * k + 64, :].astype(F32)
        slot_b[64 * k:64 * k + 64, :] = turned_b(normed_b(v, g_kb), k).astype(BF16)
    vt = vb_in[...].astype(F32).T.astype(BF16)
    slot_b[256:384, :] = vt[:, 0:128]
    slot_b[384:512, :] = vt[:, 128:256]
    pl.semaphore_wait(barrier, 15)

    g = Gather(p, lambda z, c: ba.at[c, z], lambda z, x, c: ba.at[c, z, x], lambda z, x, c: bb.at[c, z, x], sems[:n])
    w = Gather(p, lambda z, c: wa.at[pl.ds(z * NX, NX), c], lambda z, x, c: wa.at[z * NX + x, c],
               lambda z, x, c: wb.at[z * NX + x, c], sems[n:])

    g.start_a()
    g.start_b()
    inputs[6].wait()
    inputs[7].wait()
    for h in range(2):
        blocks = []
        for k in range(4):
            v = qa_in[64 * k:64 * k + 64, 128 * h:128 * h + 128].astype(F32)
            blocks.append(turned_a(normed_a(v, g_qa), k, k) * 0.125)
        qt = jnp.concatenate(blocks, axis=0).T.astype(BF16)
        qa_ref[2 * h] = qt[0:64, :]
        qa_ref[2 * h + 1] = qt[64:128, :]
    for h in range(2):
        blocks = []
        for k in range(4):
            v = qb_in[64 * k:64 * k + 64, 128 * h:128 * h + 128].astype(F32)
            blocks.append(turned_b(normed_b(v, g_qb), k))
        qb_ref[h] = jnp.concatenate(blocks, axis=0).T.astype(BF16)
    acc_a[...] = jnp.zeros_like(acc_a)
    acc_b[...] = jnp.zeros_like(acc_b)
    mx[...] = jnp.full_like(mx, -1e30)
    g.x_a1()
    g.x_a2()
    for copy in (own_g, own_ua, own_ub, own_d):
        copy.wait()
    g.x1(0)
    g.x2(0)
    g.z_b(1)
    g.z_b(2)

    zeros64 = jnp.zeros((64, 256), BF16)

    def scores(tile, buf, parts):
        top = None
        if tile < 4:
            q = qa_ref[tile]
            both = (jnp.concatenate([q, zeros64], axis=0), jnp.concatenate([zeros64, q], axis=0))
            for i, (cc, z) in enumerate(parts):
                keys = ba[cc, z, :, 0:128, :].reshape(512, 128)
                for h in range(2):
                    sc = dot(keys, both[h])
                    buf[pl.ds((i * 2 + h) * 512, 512), :] = sc
                    m8 = jnp.max(sc.reshape(64, 8, 256), axis=0)
                    top = m8 if top is None else jnp.maximum(top, m8)
        else:
            q = qb_ref[tile - 4]
            for i, (cc, z) in enumerate(parts):
                for h in range(2):
                    keys = bb[cc, z, 2 * h:2 * h + 2, 0:256, :].reshape(512, 128)
                    sc = dot(keys, q)
                    buf[pl.ds((i * 2 + h) * 512, 512), :] = sc
                    m8 = jnp.max(sc.reshape(64, 8, 256), axis=0)
                    top = m8 if top is None else jnp.maximum(top, m8)
        return jnp.max(top, axis=0, keepdims=True)

    def weigh(tile, buf, top, parts):
        scale = LOG2E if tile < 4 else LOG2E * DHB ** -0.5
        old = mx[tile]
        new = jnp.maximum(old, top * scale)
        mx[tile] = new
        factor = jnp.exp2(old - new)
        total = None
        for i, (cc, z) in enumerate(parts):
            for h in range(2):
                rows = pl.ds((i * 2 + h) * 512, 512)
                p_ref[rows, :] = jnp.exp2(buf[rows, :] * scale - new).astype(BF16)
                if tile < 4:
                    vt = jnp.concatenate([ba[cc, z, x, 128 + 64 * h:192 + 64 * h, :] for x in range(4)], axis=1)
                else:
                    vt = jnp.concatenate(
                        [bb[cc, z, x, 256 + 128 * e:384 + 128 * e, :] for x in (2 * h, 2 * h + 1) for e in range(2)], axis=1)
                vt = jnp.concatenate([vt, jnp.ones((16, 512), BF16)], axis=0)
                o = dot(vt, p_ref[rows, :])
                total = o if total is None else total + o
        if tile < 4:
            acc_a[tile] = acc_a[tile] * factor + total
        else:
            acc_b[tile - 4] = acc_b[tile - 4] * factor + total

    def both_sets(event, t):
        event(t)

        @pl.when(t + 1 < NSETS)
        def _():
            event(t + 1)

    @pl.loop(1, NSETS + 1)
    def _(t):
        odd = t % 2 == 1
        parts = ((p.c, p.set_z(t - 1, p.s)), (1 - p.c, p.set_z(t - 1, -p.s)))
        g.x3(t - 1)
        g.arrived(t - 1)

        @pl.when(odd)
        def _():
            g.x1(t)
            g.x2(t)

            @pl.when(t + 1 < NSETS)
            def _():
                g.x1(t + 1)
                g.x2(t + 1)

        bufs = (s_a, s_b)
        top = scores(0, bufs[0], parts)
        for i in range(6):
            following = scores(i + 1, bufs[(i + 1) % 2], parts) if i < 5 else None
            weigh(i, bufs[i % 2], top, parts)
            top = following
            if i == 1:
                @pl.when(odd)
                def _():
                    g.z_a(t)

                    @pl.when(t + 1 < NSETS)
                    def _():
                        g.z_a(t + 1)

                @pl.when(t == W_START)
                def _():
                    w.start_a()
                    w.start_b()
            if i == 3:
                @pl.when(t == W_FIRST - 1)
                def _():
                    w.x_a1()
                    w.x1(0)

                @pl.when(t == W_FIRST)
                def _():
                    w.x_a2()

                @pl.when(jnp.logical_and(odd, t > W_FIRST))
                def _():
                    both_sets(w.z_b, t - W_FIRST - 1)
                    both_sets(w.z_a, t - W_FIRST - 1)

                @pl.when(jnp.logical_and(jnp.logical_not(odd), t > W_FIRST + 2))
                def _():
                    both_sets(w.x1, t - W_FIRST - 2)
            if i == 5:
                @pl.when(jnp.logical_and(odd, t + 2 < NSETS))
                def _():
                    g.z_b(t + 2)

                    @pl.when(t + 3 < NSETS)
                    def _():
                        g.z_b(t + 3)

    o_a = [acc_a[h, 0:64, :] / acc_a[h, 64:65, :] for h in range(4)]
    attn[:, 0:256] = jnp.concatenate(o_a, axis=0).T.astype(BF16)
    o_b = [acc_b[h, 0:128, :] / acc_b[h, 128:129, :] for h in range(2)]
    attn[:, 256:512] = jnp.concatenate(o_b, axis=0).T.astype(BF16)
    own_oa.wait()
    own_ob.wait()
    for k in range(8):
        cols = slice(k * 256, k * 256 + 256)
        tile = dot(attn[:, 0:256], woa[:, cols]) + dot(attn[:, 256:512], wob[:, cols])
        part[:, k // 4, :, (k % 4) * 256:(k % 4) * 256 + 256] = tile.astype(BF16).reshape(4, 64, 256)

    def to_y(src, dst, s_sem, r_sem, y):
        return pltpu.make_async_remote_copy(src_ref=src, dst_ref=dst, send_sem=s_sem, recv_sem=r_sem,
                                            device_id={"tp": y}, device_id_type=MESH)

    def reduce_copies(src, mids, ins, ss, rr):
        return (
            to_y(src.at[opp, 0], mids.at[0], ss.at[0], rr.at[0], up),
            to_y(src.at[opp, 1], mids.at[1], ss.at[1], rr.at[1], down),
            to_y(src.at[down, 0], ins.at[0], ss.at[2], rr.at[2], down),
            to_y(src.at[up, 1], ins.at[1], ss.at[3], rr.at[3], up),
            to_y(mids.at[2], ins.at[2], ss.at[4], rr.at[4], up),
            to_y(mids.at[3], ins.at[3], ss.at[5], rr.at[5], down),
        )

    def reduce_first(copies):
        for copy in copies[:4]:
            copy.start()

    def reduce_second(copies, src, mids):
        copies[0].wait_recv()
        mids[2] = (src[up, 0].astype(F32) + mids[0].astype(F32)).astype(BF16)
        copies[1].wait_recv()
        mids[3] = (src[down, 1].astype(F32) + mids[1].astype(F32)).astype(BF16)
        copies[4].start()
        copies[5].start()

    def reduce_last(copies):
        for copy in copies[2:]:
            copy.wait_recv()

    first = reduce_copies(part, rs_mid, rs_in, rs_s, rs_r)
    reduce_first(first)
    left = [u for u in (1, 3, 5, 7) if u > 6 - W_FIRST + 0]

    def weights_pair(t, events):
        for event in events:
            for u in (t, t + 1):
                if u < NSETS:
                    event(u)

    for u in left[:-1]:
        weights_pair(u, (w.z_b, w.z_a))
    reduce_second(first, part, rs_mid)
    for u in left[:-1]:
        weights_pair(u, (w.x1,))
    weights_pair(7, (w.z_b, w.z_a))
    reduce_last(first)

    def own_sum(src, ins, h):
        mine = src[p.y, h].astype(F32)
        from_up, from_down = (0, 2) if h == 0 else (3, 1)
        return mine + ins[from_up].astype(F32) + ins[from_down].astype(F32)

    square = None
    for h in range(2):
        cols = slice(h * 1024, h * 1024 + 1024)
        m = x_ref[:, cols].astype(F32) + own_sum(part, rs_in, h)
        mid[:, cols] = m
        sq = jnp.sum(m * m, axis=1, keepdims=True)
        square = sq if square is None else square + sq
    inv = lax.rsqrt(square * (1.0 / 2048) + norm_eps)
    for h in range(2):
        cols = slice(h * 1024, h * 1024 + 1024)
        ag[p.y, h] = (mid[:, cols] * inv * gain_ref[:, cols]).astype(BF16)

    def ag_copy(k, d, h, y):
        return to_y(ag.at[d, h], ag.at[d, h], ag_s.at[k], ag_r.at[k], y)

    gathers = (
        ag_copy(0, p.y, 0, up), ag_copy(1, p.y, 1, down), ag_copy(2, p.y, 1, up), ag_copy(3, p.y, 0, down),
        ag_copy(4, down, 0, up), ag_copy(5, up, 1, down),
    )
    def edge_copy(k, y):
        src, sp = (ag.at[3, :, pl.ds(48, 16)], sp_next) if k == 0 else (ag.at[0, :, pl.ds(0, 16)], sp_prev)
        return pltpu.make_async_remote_copy(src_ref=src, dst_ref=edge.at[k], send_sem=h_s.at[y], recv_sem=h_r.at[k],
                                            device_id={"sp": sp, "tp": y}, device_id_type=MESH)

    for k, y in ((0, 3), (1, 0)):
        @pl.when(p.y == y)
        def _():
            for to in range(4):
                edge_copy(k, to).start()

    for copy in gathers[:4]:
        copy.start()

    weights_pair(7, (w.x1,))
    gathers[0].wait_recv()
    gathers[4].start()
    gathers[1].wait_recv()
    gathers[5].start()

    @pl.loop(0, NSETS)
    def _(t):
        w.x2(t)
        w.x3(t)

    @pl.loop(0, NSETS)
    def _(t):
        w.arrived(t)

    for copy in gathers[2:]:
        copy.wait_recv()
    edge_copy(0, 0).wait_recv()
    edge_copy(1, 0).wait_recv()
    for k, y in ((0, 3), (1, 0)):
        @pl.when(p.y == y)
        def _():
            for to in range(4):
                edge_copy(k, to).wait_send()

    rows = [jnp.concatenate([edge[0, h], ag[:, h].reshape(256, 1024), edge[1, h]], axis=0) for h in range(2)]
    for m in range(2):
        for k in range(3):
            cols = slice(k * 256, k * 256 + 256)
            tile = None
            for h in range(2):
                half = slice(16 * h, 16 * h + 16)
                if m == 0:
                    block = wa[half, :, :, cols]
                elif k == 0:
                    block = wa[half, :, :, 768:1024]
                elif k == 1:
                    block = jnp.concatenate([wa[half, :, :, 1024:1152], wb[half, :, :, 0:128]], axis=-1)
                else:
                    block = wb[half, :, :, 128:384]
                block = block.reshape(1024, 256)
                o = dot(rows[h], block)
                tile = o if tile is None else tile + o
            pre[:, m * 768 + k * 256:m * 768 + k * 256 + 256] = tile.astype(BF16)

    keep_prev = jnp.where(p.sp == 0, 0.0, 1.0).astype(F32)
    keep_next = jnp.where(p.sp == 63, 0.0, 1.0).astype(F32)
    row = lax.broadcasted_iota(jnp.int32, (256, 256), 0)
    for k in range(3):
        mixed = []
        for m, taps in ((0, cg_ref), (1, cu_ref)):
            cols = slice(m * 768 + k * 256, m * 768 + k * 256 + 256)
            tcols = slice(k * 256, k * 256 + 256)
            whole = pre[:, cols].astype(F32)
            now = whole[16:272]
            prev = jnp.where(row == 0, whole[15:16] * keep_prev, pltpu.roll(whole, 1, 0)[16:272])
            nxt = jnp.where(row == 255, whole[272:273] * keep_next, pltpu.roll(whole, 287, 0)[16:272])
            mixed.append(prev * taps[0:1, tcols] + now * taps[1:2, tcols] + nxt * taps[2:3, tcols])
        gate, upv = mixed
        hid[:, k * 256:k * 256 + 256] = (gate / (1.0 + jnp.exp(-gate)) * upv).astype(BF16)

    for k in range(8):
        block = wb[4 * k:4 * k + 4, :, :, 384:1152].reshape(256, 768)
        tile = lax.dot_general(hid[...], block, (((1,), (1,)), ((), ())), preferred_element_type=F32)
        part2[:, k // 4, :, (k % 4) * 256:(k % 4) * 256 + 256] = tile.astype(BF16).reshape(4, 64, 256)

    second = reduce_copies(part2, rs_mid2, rs_in2, rs_s2, rs_r2)
    reduce_first(second)
    g.drain()
    w.drain()
    reduce_second(second, part2, rs_mid2)
    reduce_last(second)
    for h in range(2):
        cols = slice(h * 1024, h * 1024 + 1024)
        out_ref[:, cols] = (mid[:, cols] + own_sum(part2, rs_in2, h)).astype(BF16)
    for copy in (*first, *second, *gathers):
        copy.wait_send()


def fused(*args):
    vm = pl.BlockSpec(memory_space=pltpu.VMEM)
    hb = pl.BlockSpec(memory_space=pltpu.HBM)
    v, d = pltpu.VMEM, pltpu.SemaphoreType.DMA
    scratch = [
        v((256, 256), BF16), v((64, 256), BF16), v((64, 256), BF16), v((256, 256), BF16), v((256, 128), BF16),
        v((256, 128), BF16), v((8, 128), F32), v((8, 128), F32),
        v((4, 64, 256), BF16), v((2, 128, 256), BF16),
        v((2, NZ, NX, 256, 128), BF16), v((2, NZ, NX, 512, 128), BF16),
        v((32, 2, 32, 1152), BF16), v((32, 2, 32, 1152), BF16),
        v((256, 2048), BF16), v((256, 2048), BF16),
        v((2048, 256), F32), v((2048, 256), F32), v((2048, 256), BF16),
        v((4, 80, 256), F32), v((2, 144, 256), F32), v((6, 1, 256), F32),
        v((256, 512), BF16), v((4, 2, 64, 1024), BF16), v((4, 64, 1024), BF16), v((4, 64, 1024), BF16),
        v((64, 2048), F32), v((4, 2, 64, 1024), BF16), v((288, 1536), BF16), v((2, 2, 16, 1024), BF16),
        v((256, 768), BF16), v((4, 2, 64, 1024), BF16), v((4, 64, 1024), BF16), v((4, 64, 1024), BF16),
        d((8,)), d((4,)), d((2,)), d((6,)), d((6,)), d((6,)), d((6,)), d((6,)), d((6,)), d((4,)), d((2,)),
        *gather_sems(), *gather_sems(),
    ]
    return pl.pallas_call(
        kernel,
        out_shape=jax.ShapeDtypeStruct((64, 2048), BF16),
        in_specs=[hb] * 8 + [vm] * 6 + [hb] * 5 + [vm] * 4,
        out_specs=vm,
        scratch_shapes=scratch,
        compiler_params=pltpu.CompilerParams(
            collective_id=0, has_side_effects=True, vmem_limit_bytes=60 * 1024 * 1024
        ),
        name="layer",
    )(*args)


def on_device(
    x_res, q_a, k_a, v_a, q_b, k_b, v_b, gain_qa, gain_ka, gain_qb, gain_kb,
    w_out_a, w_out_b, gain_mid, w_gate, w_up, conv_gate, conv_up, w_down,
):
    rows_a, cols_a = rotary_tables(DHA)
    rows_b, cols_b = rotary_tables(DHB)
    return fused(
        q_a, k_a.T, v_a.T, q_b, k_b, v_b, rows_a, rows_b, cols_a, cols_b,
        gain_qa[None, :], gain_ka[None, :], gain_qb[None, :], gain_kb[None, :],
        w_gate, w_up, w_down.T, w_out_a, w_out_b, x_res, gain_mid[None, :], conv_gate, conv_up,
    )


def solution(mesh):
    in_specs = (
        P(("sp", "tp"), None), P("sp", "tp"), P("sp", "tp"), P("sp", "tp"), P("sp", "tp"), P("sp", "tp"), P("sp", "tp"),
        P(), P(), P(), P(), P("tp", None), P("tp", None), P(),
        P("sp", "tp"), P("sp", "tp"), P(None, "tp"), P(None, "tp"), P("tp", "sp"),
    )
    return jax.shard_map(
        on_device, mesh=mesh, in_specs=in_specs, out_specs=P(("sp", "tp"), None), check_vma=False
    )
```

```python
import functools
import math

import jax
import jax.numpy as jnp
import numpy as np
from jax import lax
from jax.experimental import pallas as pl
from jax.experimental.pallas import tpu as pltpu
from jax.sharding import PartitionSpec as P

DHA = 64
DHB = 128
NZ = 8
NX = 4
NY = 4
NSETS = NZ
W_START = 1
W_FIRST = 3
MESH = pl.DeviceIdType.MESH
F32 = jnp.float32
BF16 = jnp.bfloat16
LOG2E = math.log2(math.e)

norm_eps = 1e-06
rope_theta = 10000.0


def rotary_tables(head_size):
    half = head_size // 2
    quarter = head_size // 4
    inverse = np.power(np.float32(rope_theta), -np.arange(0, half, 2, dtype=np.float32) / np.float32(half)).astype(np.float32)
    lane = np.arange(128)
    per_lane = inverse[lane % quarter]
    sign = np.where(lane % half < quarter, -1.0, 1.0)
    angle_r = (np.arange(256, dtype=np.float32)[:, None] * per_lane[None, :]).astype(np.float64)
    rows = np.concatenate([np.cos(angle_r).reshape(64, 4, 128), (np.sin(angle_r) * sign).reshape(64, 4, 128)], axis=1)
    angle_c = angle_r[:64]
    cols = np.stack([np.cos(angle_c), np.sin(angle_c) * sign])
    return rows.astype(np.float32), cols.astype(np.float32)


class Place:
    def __init__(self):
        self.sp = lax.axis_index("sp")
        self.y = lax.axis_index("tp")
        self.c = self.sp % 2
        self.x = (self.sp // 2) % NX
        self.z = self.sp // (2 * NX)
        self.s = 1 - 2 * self.c

    def at(self, z, x, c):
        return (z * NX + x) * 2 + c

    def zz(self, d):
        return (self.z + d + 2 * NZ) % NZ

    def xx(self, d):
        return (self.x + d + 2 * NX) % NX

    def set_z(self, t, s):
        k = (t + 1) // 2
        sign = 1 - 2 * (t % 2)
        return self.zz(sign * s * k)


class Gather:
    def __init__(self, place, group_a, piece_a, piece_b, sems):
        self.p = place
        self.group_a, self.piece_a, self.piece_b = group_a, piece_a, piece_b
        (self.ax_s, self.ax_r, self.az_s, self.az_r, self.at_s, self.at_r,
         self.bz_s, self.bz_r, self.bx_s, self.bx_r, self.bt_s, self.bt_r) = sems

    def _copy(self, ref, s_sem, r_sem, sp):
        return pltpu.make_async_remote_copy(
            src_ref=ref, dst_ref=ref, send_sem=s_sem, recv_sem=r_sem,
            device_id={"sp": sp}, device_id_type=MESH,
        )

    def c_ax(self, k):
        p = self.p
        src_x = [p.x, p.xx(-p.s), p.x][k]
        to = [p.xx(p.s), p.xx(p.s), p.xx(-p.s)][k]
        return self._copy(self.piece_a(p.z, src_x, p.c), self.ax_s.at[k], self.ax_r.at[k], p.at(p.z, to, p.c))

    def c_az(self, t, to_z, src_z):
        p = self.p
        return self._copy(self.group_a(src_z, p.c), self.az_s.at[t], self.az_r.at[t], p.at(to_z, p.x, p.c))

    def c_at(self, t):
        p = self.p
        return self._copy(self.group_a(p.set_z(t, p.s), p.c), self.at_s.at[t], self.at_r.at[t], p.at(p.z, p.x, 1 - p.c))

    def c_bz(self, t, to_z, src_z):
        p = self.p
        return self._copy(self.piece_b(src_z, p.x, p.c), self.bz_s.at[t], self.bz_r.at[t], p.at(to_z, p.x, p.c))

    def c_bx(self, t, k):
        p = self.p
        src_x = [p.x, p.xx(-p.s), p.x][k]
        to = [p.xx(p.s), p.xx(p.s), p.xx(-p.s)][k]
        return self._copy(self.piece_b(p.set_z(t, p.s), src_x, p.c), self.bx_s.at[t, k], self.bx_r.at[t, k],
                          p.at(p.z, to, p.c))

    def c_bt(self, t, k):
        p = self.p
        src_x = [p.x, p.xx(-p.s), p.xx(p.s), p.xx(-2 * p.s)][k]
        return self._copy(self.piece_b(p.set_z(t, p.s), src_x, p.c), self.bt_s.at[t, k], self.bt_r.at[t, k],
                          p.at(p.z, p.x, 1 - p.c))

    def start_b(self):
        p = self.p
        self.c_bz(1, p.zz(p.s), p.z).start()
        self.c_bz(2, p.zz(-p.s), p.z).start()
        self.c_bx(0, 0).start()
        self.c_bx(0, 2).start()
        self.c_bt(0, 0).start()

    def start_a(self):
        self.c_ax(0).start()
        self.c_ax(2).start()

    def x_a1(self):
        self.c_ax(0).wait_recv()
        self.c_ax(1).start()

    def x_a2(self):
        p = self.p
        self.c_ax(2).wait_recv()
        self.c_ax(1).wait_recv()
        self.c_az(1, p.zz(p.s), p.z).start()
        self.c_az(2, p.zz(-p.s), p.z).start()
        self.c_at(0).start()

    def _hop(self, t, copy):
        p = self.p
        sign = (2 * (t % 2) - 1) * p.s
        copy(t, p.z, p.set_z(t, p.s)).wait_recv()

        @pl.when(t <= NSETS - 3)
        def _():
            copy(t + 2, p.zz(sign), p.set_z(t, p.s)).start()

    def z_b(self, t):
        self._hop(t, self.c_bz)
        self.c_bx(t, 0).start()
        self.c_bx(t, 2).start()
        self.c_bt(t, 0).start()

    def z_a(self, t):
        self._hop(t, self.c_az)
        self.c_at(t).start()

    def x1(self, t):
        self.c_bx(t, 0).wait_recv()
        self.c_bx(t, 1).start()
        self.c_bt(t, 1).start()

    def x2(self, t):
        self.c_bx(t, 2).wait_recv()
        self.c_bt(t, 2).start()

    def x3(self, t):
        self.c_bx(t, 1).wait_recv()
        self.c_bt(t, 3).start()

    def arrived(self, t):
        self.c_at(t).wait_recv()
        for k in range(4):
            self.c_bt(t, k).wait_recv()

    def drain(self):
        p = self.p
        for k in range(3):
            self.c_ax(k).wait_send()

        @pl.loop(0, NSETS)
        def _(t):
            self.c_at(t).wait_send()
            for k in range(3):
                self.c_bx(t, k).wait_send()
            for k in range(4):
                self.c_bt(t, k).wait_send()

            @pl.when(t >= 1)
            def _():
                self.c_az(t, p.z, p.z).wait_send()
                self.c_bz(t, p.z, p.z).wait_send()


def gather_sems():
    d = pltpu.SemaphoreType.DMA
    return [d((3,)), d((3,)), d((8,)), d((8,)), d((8,)), d((8,)),
            d((8,)), d((8,)), d((8, 3)), d((8, 3)), d((8, 4)), d((8, 4))]


def dot(a, b):
    return jnp.dot(a, b, preferred_element_type=F32)


def kernel(q_a, k_a, v_a, q_b, k_b, v_b, ra_h, rb_h, col_a, col_b, g_qa, g_ka, g_qb, g_kb, wg_h, wu_h, wd_h, woa_h, wob_h, x_ref, gain_ref, cg_ref, cu_ref, out_ref,
           qa_in, ka_in, va_in, qb_in, kb_in, vb_in, ra, rb, qa_ref, qb_ref, ba, bb, wa, wb, woa, wob, s_a, s_b, p_ref, acc_a, acc_b, mx,
           attn, part, rs_mid, rs_in, mid, ag, pre, edge, hid, part2, rs_mid2, rs_in2,
           in_sem, loc, wo_sem, rs_s, rs_r, rs_s2, rs_r2, ag_s, ag_r, h_s, h_r, *sems):
    p = Place()
    n = len(sems) // 2

    barrier = pltpu.get_barrier_semaphore()
    up, down = (p.y + 1) % NY, (p.y + NY - 1) % NY
    opp = (p.y + 2) % NY
    sp_next, sp_prev = (p.sp + 1) % 64, (p.sp + 63) % 64
    pairs = ((k_a, ka_in), (v_a, va_in), (k_b, kb_in), (v_b, vb_in), (ra_h.at[p.sp], ra), (rb_h.at[p.sp], rb),
             (q_a, qa_in), (q_b, qb_in))
    inputs = [pltpu.make_async_copy(src, dst, in_sem.at[i]) for i, (src, dst) in enumerate(pairs)]
    for copy in inputs:
        copy.start()
    zx = p.z * NX + p.x
    own_g = pltpu.make_async_copy(wg_h, wa.at[zx, p.c, :, pl.ds(0, 768)], loc.at[0])
    own_ua = pltpu.make_async_copy(wu_h.at[:, pl.ds(0, 384)], wa.at[zx, p.c, :, pl.ds(768, 384)], loc.at[1])
    own_ub = pltpu.make_async_copy(wu_h.at[:, pl.ds(384, 384)], wb.at[zx, p.c, :, pl.ds(0, 384)], loc.at[2])
    own_d = pltpu.make_async_copy(wd_h, wb.at[zx, p.c, :, pl.ds(384, 768)], loc.at[3])
    own_oa = pltpu.make_async_copy(woa_h, woa, wo_sem.at[0])
    own_ob = pltpu.make_async_copy(wob_h, wob, wo_sem.at[1])
    for copy in (own_g, own_ua, own_ub, own_d, own_oa, own_ob):
        copy.start()
    greeted = [p.at(p.zz(1), p.x, p.c), p.at(p.zz(-1), p.x, p.c), p.at(p.z, p.xx(1), p.c), p.at(p.z, p.xx(-1), p.c),
               p.at(p.z, p.x, 1 - p.c), sp_next, sp_prev]
    for sp in greeted:
        pl.semaphore_signal(barrier, inc=1, device_id={"sp": sp}, device_id_type=MESH)
    for y in (up, down):
        pl.semaphore_signal(barrier, inc=1, device_id={"tp": y}, device_id_type=MESH)
    for sp in (sp_next, sp_prev):
        for y in (up, down, opp):
            pl.semaphore_signal(barrier, inc=1, device_id={"sp": sp, "tp": y}, device_id_type=MESH)

    lane = lax.broadcasted_iota(jnp.int32, (64, 128), 1)
    first_head = lane < 64

    def normed_a(v, gain):
        sq = v * v
        left = jnp.sum(jnp.where(first_head, sq, 0.0), axis=1, keepdims=True)
        right = jnp.sum(jnp.where(first_head, 0.0, sq), axis=1, keepdims=True)
        inv = lax.rsqrt(jnp.where(first_head, left, right) * (1.0 / DHA) + norm_eps)
        gains = jnp.concatenate([gain[...], gain[...]], axis=1)
        return v * inv * gains

    def normed_b(v, gain):
        inv = lax.rsqrt(jnp.sum(v * v, axis=1, keepdims=True) * (1.0 / DHB) + norm_eps)
        return v * inv * gain[...]

    def turned(v, quarter, cos, sin):
        other = jnp.where(lane % (2 * quarter) < quarter, pltpu.roll(v, 128 - quarter, 1), pltpu.roll(v, quarter, 1))
        return v * cos + other * sin

    def turned_a(v, left, right):
        row_lane = lane % 64 < 32

        def table(k):
            row = jnp.where(first_head, ra[4 * k + left:4 * k + left + 1, :], ra[4 * k + right:4 * k + right + 1, :])
            return jnp.where(row_lane, row, col_a[k])

        return turned(v, 16, table(0), table(1))

    def turned_b(v, block):
        def table(k):
            return jnp.where(first_head, rb[4 * k + block:4 * k + block + 1, :], col_b[k])

        return turned(v, 32, table(0), table(1))

    for copy in inputs[:6]:
        copy.wait()
    slot_a, slot_b = ba.at[p.c, p.z, p.x], bb.at[p.c, p.z, p.x]
    ka = ka_in[...].astype(F32).T
    for k in range(2):
        v = jnp.concatenate([ka[64 * k:64 * k + 64, :], ka[128 + 64 * k:192 + 64 * k, :]], axis=1)
        slot_a[64 * k:64 * k + 64, :] = turned_a(normed_a(v, g_ka), k, k + 2).astype(BF16)
    slot_a[128:192, :] = va_in[:, 0:128]
    slot_a[192:256, :] = va_in[:, 128:256]
    for k in range(4):
        v = kb_in[64 * k:64 * k + 64, :].astype(F32)
        slot_b[64 * k:64 * k + 64, :] = turned_b(normed_b(v, g_kb), k).astype(BF16)
    vt = vb_in[...].astype(F32).T.astype(BF16)
    slot_b[256:384, :] = vt[:, 0:128]
    slot_b[384:512, :] = vt[:, 128:256]
    pl.semaphore_wait(barrier, 15)

    g = Gather(p, lambda z, c: ba.at[c, z], lambda z, x, c: ba.at[c, z, x], lambda z, x, c: bb.at[c, z, x], sems[:n])
    w = Gather(p, lambda z, c: wa.at[pl.ds(z * NX, NX), c], lambda z, x, c: wa.at[z * NX + x, c],
               lambda z, x, c: wb.at[z * NX + x, c], sems[n:])

    g.start_a()
    g.start_b()
    inputs[6].wait()
    inputs[7].wait()
    for h in range(2):
        blocks = []
        for k in range(4):
            v = qa_in[64 * k:64 * k + 64, 128 * h:128 * h + 128].astype(F32)
            blocks.append(turned_a(normed_a(v, g_qa), k, k) * 0.125)
        qt = jnp.concatenate(blocks, axis=0).T.astype(BF16)
        qa_ref[2 * h] = qt[0:64, :]
        qa_ref[2 * h + 1] = qt[64:128, :]
    for h in range(2):
        blocks = []
        for k in range(4):
            v = qb_in[64 * k:64 * k + 64, 128 * h:128 * h + 128].astype(F32)
            blocks.append(turned_b(normed_b(v, g_qb), k))
        qb_ref[h] = jnp.concatenate(blocks, axis=0).T.astype(BF16)
    acc_a[...] = jnp.zeros_like(acc_a)
    acc_b[...] = jnp.zeros_like(acc_b)
    mx[...] = jnp.full_like(mx, -1e30)
    g.x_a1()
    g.x1(0)
    g.x_a2()
    for copy in (own_g, own_ua, own_ub, own_d):
        copy.wait()
    g.x2(0)
    g.z_b(1)
    g.z_b(2)

    zeros64 = jnp.zeros((64, 256), BF16)

    def scores(tile, buf, parts):
        top = None
        if tile < 4:
            q = qa_ref[tile]
            both = (jnp.concatenate([q, zeros64], axis=0), jnp.concatenate([zeros64, q], axis=0))
            for i, (cc, z) in enumerate(parts):
                keys = ba[cc, z, :, 0:128, :].reshape(512, 128)
                for h in range(2):
                    sc = dot(keys, both[h])
                    buf[pl.ds((i * 2 + h) * 512, 512), :] = sc
                    m8 = jnp.max(sc.reshape(64, 8, 256), axis=0)
                    top = m8 if top is None else jnp.maximum(top, m8)
        else:
            q = qb_ref[tile - 4]
            for i, (cc, z) in enumerate(parts):
                for h in range(2):
                    keys = bb[cc, z, 2 * h:2 * h + 2, 0:256, :].reshape(512, 128)
                    sc = dot(keys, q)
                    buf[pl.ds((i * 2 + h) * 512, 512), :] = sc
                    m8 = jnp.max(sc.reshape(64, 8, 256), axis=0)
                    top = m8 if top is None else jnp.maximum(top, m8)
        return jnp.max(top, axis=0, keepdims=True)

    def weigh(tile, buf, top, parts):
        scale = LOG2E if tile < 4 else LOG2E * DHB ** -0.5
        old = mx[tile]
        new = jnp.maximum(old, top * scale)
        mx[tile] = new
        factor = jnp.exp2(old - new)
        total = None
        for i, (cc, z) in enumerate(parts):
            for h in range(2):
                rows = pl.ds((i * 2 + h) * 512, 512)
                p_ref[rows, :] = jnp.exp2(buf[rows, :] * scale - new).astype(BF16)
                if tile < 4:
                    vt = jnp.concatenate([ba[cc, z, x, 128 + 64 * h:192 + 64 * h, :] for x in range(4)], axis=1)
                else:
                    vt = jnp.concatenate(
                        [bb[cc, z, x, 256 + 128 * e:384 + 128 * e, :] for x in (2 * h, 2 * h + 1) for e in range(2)], axis=1)
                vt = jnp.concatenate([vt, jnp.ones((16, 512), BF16)], axis=0)
                o = dot(vt, p_ref[rows, :])
                total = o if total is None else total + o
        if tile < 4:
            acc_a[tile] = acc_a[tile] * factor + total
        else:
            acc_b[tile - 4] = acc_b[tile - 4] * factor + total

    def both_sets(event, t):
        event(t)

        @pl.when(t + 1 < NSETS)
        def _():
            event(t + 1)

    @pl.loop(1, NSETS + 1)
    def _(t):
        odd = t % 2 == 1
        parts = ((p.c, p.set_z(t - 1, p.s)), (1 - p.c, p.set_z(t - 1, -p.s)))
        g.x3(t - 1)
        g.arrived(t - 1)

        bufs = (s_a, s_b)
        top = scores(0, bufs[0], parts)
        for i in range(6):
            following = scores(i + 1, bufs[(i + 1) % 2], parts) if i < 5 else None
            weigh(i, bufs[i % 2], top, parts)
            top = following
            if i == 0:
                @pl.when(odd)
                def _():
                    g.x1(t)
                    g.x2(t)

                    @pl.when(t + 1 < NSETS)
                    def _():
                        g.x1(t + 1)
                        g.x2(t + 1)

                @pl.when(t == W_START)
                def _():
                    w.start_a()
                    w.start_b()

            if i == 1:
                @pl.when(odd)
                def _():
                    g.z_a(t)

                    @pl.when(t + 1 < NSETS)
                    def _():
                        g.z_a(t + 1)

            if i == 2:
                @pl.when(t == W_FIRST - 1)
                def _():
                    w.x_a1()
                    w.x1(0)

                @pl.when(t == W_FIRST)
                def _():
                    w.x_a2()

            if i == 3:
                @pl.when(jnp.logical_and(odd, t > W_FIRST))
                def _():
                    both_sets(w.z_b, t - W_FIRST - 1)
                    both_sets(w.z_a, t - W_FIRST - 1)

            if i == 4:
                @pl.when(jnp.logical_and(jnp.logical_not(odd), t > W_FIRST + 2))
                def _():
                    both_sets(w.x1, t - W_FIRST - 2)

            if i == 5:
                @pl.when(jnp.logical_and(odd, t + 2 < NSETS))
                def _():
                    g.z_b(t + 2)

                    @pl.when(t + 3 < NSETS)
                    def _():
                        g.z_b(t + 3)

    o_a = [acc_a[h, 0:64, :] / acc_a[h, 64:65, :] for h in range(4)]
    attn[:, 0:256] = jnp.concatenate(o_a, axis=0).T.astype(BF16)
    o_b = [acc_b[h, 0:128, :] / acc_b[h, 128:129, :] for h in range(2)]
    attn[:, 256:512] = jnp.concatenate(o_b, axis=0).T.astype(BF16)
    own_oa.wait()
    own_ob.wait()
    for k in range(8):
        cols = slice(k * 256, k * 256 + 256)
        tile = dot(attn[:, 0:256], woa[:, cols]) + dot(attn[:, 256:512], wob[:, cols])
        part[:, k // 4, :, (k % 4) * 256:(k % 4) * 256 + 256] = tile.astype(BF16).reshape(4, 64, 256)

    def to_y(src, dst, s_sem, r_sem, y):
        return pltpu.make_async_remote_copy(src_ref=src, dst_ref=dst, send_sem=s_sem, recv_sem=r_sem,
                                            device_id={"tp": y}, device_id_type=MESH)

    def reduce_copies(src, mids, ins, ss, rr):
        return (
            to_y(src.at[opp, 0], mids.at[0], ss.at[0], rr.at[0], up),
            to_y(src.at[opp, 1], mids.at[1], ss.at[1], rr.at[1], down),
            to_y(src.at[down, 0], ins.at[0], ss.at[2], rr.at[2], down),
            to_y(src.at[up, 1], ins.at[1], ss.at[3], rr.at[3], up),
            to_y(mids.at[2], ins.at[2], ss.at[4], rr.at[4], up),
            to_y(mids.at[3], ins.at[3], ss.at[5], rr.at[5], down),
        )

    def reduce_first(copies):
        for copy in copies[:4]:
            copy.start()

    def reduce_second(copies, src, mids):
        copies[0].wait_recv()
        mids[2] = (src[up, 0].astype(F32) + mids[0].astype(F32)).astype(BF16)
        copies[1].wait_recv()
        mids[3] = (src[down, 1].astype(F32) + mids[1].astype(F32)).astype(BF16)
        copies[4].start()
        copies[5].start()

    def reduce_last(copies):
        for copy in copies[2:]:
            copy.wait_recv()

    first = reduce_copies(part, rs_mid, rs_in, rs_s, rs_r)
    reduce_first(first)
    left = [u for u in (1, 3, 5, 7) if u > 6 - W_FIRST + 0]

    def weights_pair(t, events):
        for event in events:
            for u in (t, t + 1):
                if u < NSETS:
                    event(u)

    for u in left[:-1]:
        weights_pair(u, (w.z_b, w.z_a))
    reduce_second(first, part, rs_mid)
    for u in left[:-1]:
        weights_pair(u, (w.x1,))
    reduce_last(first)

    def own_sum(src, ins, h):
        mine = src[p.y, h].astype(F32)
        from_up, from_down = (0, 2) if h == 0 else (3, 1)
        return mine + ins[from_up].astype(F32) + ins[from_down].astype(F32)

    square = None
    for h in range(2):
        cols = slice(h * 1024, h * 1024 + 1024)
        m = x_ref[:, cols].astype(F32) + own_sum(part, rs_in, h)
        mid[:, cols] = m
        sq = jnp.sum(m * m, axis=1, keepdims=True)
        square = sq if square is None else square + sq
    inv = lax.rsqrt(square * (1.0 / 2048) + norm_eps)
    for h in range(2):
        cols = slice(h * 1024, h * 1024 + 1024)
        ag[p.y, h] = (mid[:, cols] * inv * gain_ref[:, cols]).astype(BF16)

    def ag_copy(k, d, h, y):
        return to_y(ag.at[d, h], ag.at[d, h], ag_s.at[k], ag_r.at[k], y)

    gathers = (
        ag_copy(0, p.y, 0, up), ag_copy(1, p.y, 1, down), ag_copy(2, p.y, 1, up), ag_copy(3, p.y, 0, down),
        ag_copy(4, down, 0, up), ag_copy(5, up, 1, down),
    )
    def edge_copy(k, y):
        src, sp = (ag.at[3, :, pl.ds(48, 16)], sp_next) if k == 0 else (ag.at[0, :, pl.ds(0, 16)], sp_prev)
        return pltpu.make_async_remote_copy(src_ref=src, dst_ref=edge.at[k], send_sem=h_s.at[y], recv_sem=h_r.at[k],
                                            device_id={"sp": sp, "tp": y}, device_id_type=MESH)

    for k, y in ((0, 3), (1, 0)):
        @pl.when(p.y == y)
        def _():
            for to in range(4):
                edge_copy(k, to).start()

    for copy in gathers[:4]:
        copy.start()

    weights_pair(7, (w.z_b, w.z_a))
    gathers[0].wait_recv()
    gathers[4].start()
    gathers[1].wait_recv()
    gathers[5].start()
    weights_pair(7, (w.x1,))

    @pl.loop(0, NSETS)
    def _(t):
        w.x2(t)
        w.x3(t)

    @pl.loop(0, NSETS)
    def _(t):
        w.arrived(t)

    for copy in gathers[2:]:
        copy.wait_recv()
    edge_copy(0, 0).wait_recv()
    edge_copy(1, 0).wait_recv()
    for k, y in ((0, 3), (1, 0)):
        @pl.when(p.y == y)
        def _():
            for to in range(4):
                edge_copy(k, to).wait_send()

    rows = [jnp.concatenate([edge[0, h], ag[:, h].reshape(256, 1024), edge[1, h]], axis=0) for h in range(2)]
    for m in range(2):
        for k in range(3):
            cols = slice(k * 256, k * 256 + 256)
            tile = None
            for h in range(2):
                half = slice(16 * h, 16 * h + 16)
                if m == 0:
                    block = wa[half, :, :, cols]
                elif k == 0:
                    block = wa[half, :, :, 768:1024]
                elif k == 1:
                    block = jnp.concatenate([wa[half, :, :, 1024:1152], wb[half, :, :, 0:128]], axis=-1)
                else:
                    block = wb[half, :, :, 128:384]
                block = block.reshape(1024, 256)
                o = dot(rows[h], block)
                tile = o if tile is None else tile + o
            pre[:, m * 768 + k * 256:m * 768 + k * 256 + 256] = tile.astype(BF16)

    keep_prev = jnp.where(p.sp == 0, 0.0, 1.0).astype(F32)
    keep_next = jnp.where(p.sp == 63, 0.0, 1.0).astype(F32)
    row = lax.broadcasted_iota(jnp.int32, (256, 256), 0)
    for k in range(3):
        mixed = []
        for m, taps in ((0, cg_ref), (1, cu_ref)):
            cols = slice(m * 768 + k * 256, m * 768 + k * 256 + 256)
            tcols = slice(k * 256, k * 256 + 256)
            whole = pre[:, cols].astype(F32)
            now = whole[16:272]
            prev = jnp.where(row == 0, whole[15:16] * keep_prev, pltpu.roll(whole, 1, 0)[16:272])
            nxt = jnp.where(row == 255, whole[272:273] * keep_next, pltpu.roll(whole, 287, 0)[16:272])
            mixed.append(prev * taps[0:1, tcols] + now * taps[1:2, tcols] + nxt * taps[2:3, tcols])
        gate, upv = mixed
        hid[:, k * 256:k * 256 + 256] = (gate / (1.0 + jnp.exp(-gate)) * upv).astype(BF16)

    for k in range(8):
        block = wb[4 * k:4 * k + 4, :, :, 384:1152].reshape(256, 768)
        tile = lax.dot_general(hid[...], block, (((1,), (1,)), ((), ())), preferred_element_type=F32)
        part2[:, k // 4, :, (k % 4) * 256:(k % 4) * 256 + 256] = tile.astype(BF16).reshape(4, 64, 256)

    second = reduce_copies(part2, rs_mid2, rs_in2, rs_s2, rs_r2)
    reduce_first(second)
    g.drain()
    w.drain()
    reduce_second(second, part2, rs_mid2)
    reduce_last(second)
    for h in range(2):
        cols = slice(h * 1024, h * 1024 + 1024)
        out_ref[:, cols] = (mid[:, cols] + own_sum(part2, rs_in2, h)).astype(BF16)
    for copy in (*first, *second, *gathers):
        copy.wait_send()


def fused(*args):
    vm = pl.BlockSpec(memory_space=pltpu.VMEM)
    hb = pl.BlockSpec(memory_space=pltpu.HBM)
    v, d = pltpu.VMEM, pltpu.SemaphoreType.DMA
    scratch = [
        v((256, 256), BF16), v((64, 256), BF16), v((64, 256), BF16), v((256, 256), BF16), v((256, 128), BF16),
        v((256, 128), BF16), v((8, 128), F32), v((8, 128), F32),
        v((4, 64, 256), BF16), v((2, 128, 256), BF16),
        v((2, NZ, NX, 256, 128), BF16), v((2, NZ, NX, 512, 128), BF16),
        v((32, 2, 32, 1152), BF16), v((32, 2, 32, 1152), BF16),
        v((256, 2048), BF16), v((256, 2048), BF16),
        v((2048, 256), F32), v((2048, 256), F32), v((2048, 256), BF16),
        v((4, 80, 256), F32), v((2, 144, 256), F32), v((6, 1, 256), F32),
        v((256, 512), BF16), v((4, 2, 64, 1024), BF16), v((4, 64, 1024), BF16), v((4, 64, 1024), BF16),
        v((64, 2048), F32), v((4, 2, 64, 1024), BF16), v((288, 1536), BF16), v((2, 2, 16, 1024), BF16),
        v((256, 768), BF16), v((4, 2, 64, 1024), BF16), v((4, 64, 1024), BF16), v((4, 64, 1024), BF16),
        d((8,)), d((4,)), d((2,)), d((6,)), d((6,)), d((6,)), d((6,)), d((6,)), d((6,)), d((4,)), d((2,)),
        *gather_sems(), *gather_sems(),
    ]
    return pl.pallas_call(
        kernel,
        out_shape=jax.ShapeDtypeStruct((64, 2048), BF16),
        in_specs=[hb] * 8 + [vm] * 6 + [hb] * 5 + [vm] * 4,
        out_specs=vm,
        scratch_shapes=scratch,
        compiler_params=pltpu.CompilerParams(
            collective_id=0, has_side_effects=True, vmem_limit_bytes=60 * 1024 * 1024
        ),
        name="layer",
    )(*args)


def on_device(
    x_res, q_a, k_a, v_a, q_b, k_b, v_b, gain_qa, gain_ka, gain_qb, gain_kb,
    w_out_a, w_out_b, gain_mid, w_gate, w_up, conv_gate, conv_up, w_down,
):
    rows_a, cols_a = rotary_tables(DHA)
    rows_b, cols_b = rotary_tables(DHB)
    return fused(
        q_a, k_a.T, v_a.T, q_b, k_b, v_b, rows_a, rows_b, cols_a, cols_b,
        gain_qa[None, :], gain_ka[None, :], gain_qb[None, :], gain_kb[None, :],
        w_gate, w_up, w_down.T, w_out_a, w_out_b, x_res, gain_mid[None, :], conv_gate, conv_up,
    )


def solution(mesh):
    in_specs = (
        P(("sp", "tp"), None), P("sp", "tp"), P("sp", "tp"), P("sp", "tp"), P("sp", "tp"), P("sp", "tp"), P("sp", "tp"),
        P(), P(), P(), P(), P("tp", None), P("tp", None), P(),
        P("sp", "tp"), P("sp", "tp"), P(None, "tp"), P(None, "tp"), P("tp", "sp"),
    )
    return jax.shard_map(
        on_device, mesh=mesh, in_specs=in_specs, out_specs=P(("sp", "tp"), None), check_vma=False
    )
```
